512 devices in a mesh: sp: 32 (over z, x), dp: 16 (over y, core).
Axes of the slice: x: 4, y: 8, z: 8, core: 2. Of those that a mesh axis runs over, the one named last changes fastest.
Arguments:
- inputs: bfloat16 [6144, 2048], P('sp'), may hold values from -6 to 6
- w_query: bfloat16 [2048, 2048], P('dp'), may hold values from -0.125 to 0.125
- w_key: bfloat16 [1024, 2048], P('dp'), may hold values from -0.125 to 0.125
- w_value: bfloat16 [1024, 2048], P('dp'), may hold values from -0.125 to 0.125
- query_gain: float32 [64], replicated, may hold values from 0.6 to 7
- key_gain: float32 [64], replicated, may hold values from 0.6 to 7
- grad_out: bfloat16 [6144, 2048], P('sp', 'dp'), may hold values from -6 to 6
Outputs:
- d_inputs: bfloat16 [6144, 2048], P('sp', 'dp')
- grad_wq: float32 [2048, 2048], P('dp')
- grad_wk: float32 [1024, 2048], P('dp')
- grad_wv: float32 [1024, 2048], P('dp')
The draws below stay inside these ranges and needn't reach their ends.
All inputs are finite; a program needn't handle non-finite values.
Results may differ from the reference program's by a relative error of at most 0.019.
The reference program's roundings to bfloat16 on the way count: a program that leaves them out, or rounds other values in their place, can miss the bound.
Values may be sent and summed in bfloat16 or wider, within the bound.
A program may use at most 64 MiB of HBM per device.

```python
import math
import jax
import jax.numpy as jnp
from jax import lax

D = 2048
HEAD_WIDTH = 64
QHEADS = 32
KEY_VALUE_HEADS = 16
GRID_W = 64
SEQUENCE_TOKENS = 6144
N_DP = 16


def gain_values(key):
    return jnp.exp(jax.random.uniform(key, (HEAD_WIDTH,), jnp.float32, math.log(0.6), math.log(1.6)))


def draw_query_gain(key, part):
    return gain_values(jax.random.fold_in(key, 31))


def draw_key_gain(key, part):
    return gain_values(jax.random.fold_in(key, 47))


def levels(key, shape, cuts, least, high):
    level = 1.0
    for position, blocks in cuts:
        draws = jax.random.uniform(jax.random.fold_in(jax.random.fold_in(key, 6), position), (blocks,), jnp.float32, least / len(cuts), high / len(cuts))
        level = level * jnp.repeat(jnp.exp(draws), shape[position] // blocks).reshape((-1,) + (1,) * (len(shape) - 1 - position))
    return level


def gaussian(stream_key, dims, scale, reach, split=(), kind=jnp.bfloat16):
    values = scale * jax.random.normal(stream_key, dims, jnp.float32)
    if split:
        values = values * levels(stream_key, dims, split, -0.22, 0.18)
    return jnp.clip(values, -reach, reach).astype(kind)


def setup_inputs(seed: int = 0) -> dict:
    arg_keys = jax.random.split(jax.random.key(seed), 8)
    return {
        "inputs": gaussian(arg_keys[0], (SEQUENCE_TOKENS, D), 1.0, 6.0, ((0, 32),)),
        "w_query": gaussian(arg_keys[1], (QHEADS * HEAD_WIDTH, D), D ** -0.5, 0.125, ((0, 16),)),
        "w_key": gaussian(arg_keys[2], (KEY_VALUE_HEADS * HEAD_WIDTH, D), D ** -0.5, 0.125, ((0, 16),)),
        "w_value": gaussian(arg_keys[3], (KEY_VALUE_HEADS * HEAD_WIDTH, D), D ** -0.5, 0.125, ((0, 16),)),
        "query_gain": draw_query_gain(jax.random.fold_in(arg_keys[7], 71), 0),
        "key_gain": draw_key_gain(jax.random.fold_in(arg_keys[7], 71), 0),
        "grad_out": gaussian(arg_keys[6], (SEQUENCE_TOKENS, QHEADS * HEAD_WIDTH), 1.0, 6.0, ((0, 32), (1, 16))),
    }


norm_eps = 1e-06
axial_base = 10000.0

def rotation_tables(offset, count):
    positions = offset + jnp.arange(count, dtype=jnp.int32)
    grid_rows = (positions // GRID_W).astype(jnp.float32)
    grid_cols = (positions % GRID_W).astype(jnp.float32)
    quarter = HEAD_WIDTH // 4
    freqs_axis = axial_base ** (-jnp.arange(quarter, dtype=jnp.float32) / quarter)
    angle_rows = grid_rows[:, None] * freqs_axis[None, :]
    angle_cols = grid_cols[:, None] * freqs_axis[None, :]
    cosine = jnp.concatenate([jnp.cos(angle_rows), jnp.cos(angle_rows), jnp.cos(angle_cols), jnp.cos(angle_cols)], axis=1)
    sine = jnp.concatenate([jnp.sin(angle_rows), jnp.sin(angle_rows), jnp.sin(angle_cols), jnp.sin(angle_cols)], axis=1)
    return (cosine, sine)

def quarter_turn(values):
    quarter = HEAD_WIDTH // 4
    return jnp.concatenate([-values[..., quarter:2 * quarter], values[..., :quarter], -values[..., 3 * quarter:], values[..., 2 * quarter:3 * quarter]], axis=-1)

def quarter_back(values):
    quarter = HEAD_WIDTH // 4
    return jnp.concatenate([values[..., quarter:2 * quarter], -values[..., :quarter], values[..., 3 * quarter:], -values[..., 2 * quarter:3 * quarter]], axis=-1)

def rotate(values, cosine, sine):
    return values * cosine + quarter_turn(values) * sine

def rotate_back(grads, cosine, sine):
    return grads * cosine + quarter_back(grads * sine)

def head_norm(raw):
    scale_inv = lax.rsqrt(lax.optimization_barrier(jnp.mean(raw * raw, axis=-1, keepdims=True)) + norm_eps)
    return (raw * scale_inv, scale_inv)

def head_norm_back(grads, normed, scale_inv, gain):
    scaled = grads * gain
    return scale_inv * (scaled - normed * lax.optimization_barrier(jnp.mean(scaled * normed, axis=-1, keepdims=True)))

def reference(inputs, w_query, w_key, w_value, query_gain, key_gain, grad_out):
    group = QHEADS // KEY_VALUE_HEADS
    scale = HEAD_WIDTH ** (-0.5)
    cosine, sine = rotation_tables(0, SEQUENCE_TOKENS)
    cos_wide = cosine[:, None, :]
    sin_wide = sine[:, None, :]
    q_raw = jnp.dot(inputs, w_query.T, preferred_element_type=jnp.float32).astype(jnp.bfloat16)
    k_raw = jnp.dot(inputs, w_key.T, preferred_element_type=jnp.float32).astype(jnp.bfloat16)
    v_raw = jnp.dot(inputs, w_value.T, preferred_element_type=jnp.float32).astype(jnp.bfloat16)
    q_wide = lax.optimization_barrier(q_raw).astype(jnp.float32).reshape(SEQUENCE_TOKENS, QHEADS, HEAD_WIDTH)
    k_wide = lax.optimization_barrier(k_raw).astype(jnp.float32).reshape(SEQUENCE_TOKENS, KEY_VALUE_HEADS, HEAD_WIDTH)
    q_normed, q_inv = head_norm(q_wide)
    k_normed, k_inv = head_norm(k_wide)
    q_rot = rotate(q_normed * query_gain, cos_wide, sin_wide).astype(jnp.bfloat16)
    k_rot = rotate(k_normed * key_gain, cos_wide, sin_wide).astype(jnp.bfloat16)
    query_heads = q_rot.reshape(SEQUENCE_TOKENS, KEY_VALUE_HEADS, group, HEAD_WIDTH).transpose(1, 0, 2, 3)
    gradient_heads = grad_out.reshape(SEQUENCE_TOKENS, KEY_VALUE_HEADS, group, HEAD_WIDTH).transpose(1, 0, 2, 3)
    key_heads = k_rot.transpose(1, 0, 2)
    value_heads = v_raw.reshape(SEQUENCE_TOKENS, KEY_VALUE_HEADS, HEAD_WIDTH).transpose(1, 0, 2)

    def single_key_head(operands):
        query_rot, key_rot, value_rows, grad_rows = operands
        grad_query = []
        grad_key = jnp.zeros((SEQUENCE_TOKENS, HEAD_WIDTH), jnp.float32)
        grad_value = jnp.zeros((SEQUENCE_TOKENS, HEAD_WIDTH), jnp.float32)
        for member in range(group):
            query_head = query_rot[:, member]
            grad_head = grad_rows[:, member]
            scores = jnp.dot(query_head, key_rot.T, preferred_element_type=jnp.float32) * scale
            maxima = lax.optimization_barrier(jnp.max(scores, axis=1, keepdims=True))
            log_total = maxima + jnp.log(lax.optimization_barrier(jnp.sum(jnp.exp(scores - maxima), axis=1, keepdims=True)))
            prob_exact = jnp.exp(scores - log_total)
            prob_half = prob_exact.astype(jnp.bfloat16)
            attn_rows = jnp.dot(prob_half, value_rows, preferred_element_type=jnp.float32).astype(jnp.bfloat16)
            attn_wide = lax.optimization_barrier(attn_rows).astype(jnp.float32)
            delta_rows = lax.optimization_barrier(jnp.sum(grad_head.astype(jnp.float32) * attn_wide, axis=1, keepdims=True))
            grad_value = grad_value + jnp.dot(prob_half.T, grad_head, preferred_element_type=jnp.float32)
            dprob = jnp.dot(grad_head, value_rows.T, preferred_element_type=jnp.float32)
            dscore = (prob_exact * (dprob - delta_rows)).astype(jnp.bfloat16)
            grad_query.append(jnp.dot(dscore, key_rot, preferred_element_type=jnp.float32) * scale)
            grad_key = grad_key + jnp.dot(dscore.T, query_head, preferred_element_type=jnp.float32) * scale
        return (jnp.stack(grad_query, axis=1), grad_key, grad_value)
    gradient_query_rotated, gradient_key_rotated, gradient_value_rotated = lax.map(single_key_head, (query_heads, key_heads, value_heads, gradient_heads))
    gradient_query_rotated = gradient_query_rotated.transpose(1, 0, 2, 3).reshape(SEQUENCE_TOKENS, QHEADS, HEAD_WIDTH)
    gradient_key_rotated = gradient_key_rotated.transpose(1, 0, 2)
    gradient_values = gradient_value_rotated.transpose(1, 0, 2).reshape(SEQUENCE_TOKENS, KEY_VALUE_HEADS * HEAD_WIDTH).astype(jnp.bfloat16)
    grad_q = head_norm_back(rotate_back(gradient_query_rotated, cos_wide, sin_wide), q_normed, q_inv, query_gain)
    grad_q = grad_q.reshape(SEQUENCE_TOKENS, QHEADS * HEAD_WIDTH).astype(jnp.bfloat16)
    grad_k = head_norm_back(rotate_back(gradient_key_rotated, cos_wide, sin_wide), k_normed, k_inv, key_gain)
    grad_k = grad_k.reshape(SEQUENCE_TOKENS, KEY_VALUE_HEADS * HEAD_WIDTH).astype(jnp.bfloat16)
    query_cols = QHEADS * HEAD_WIDTH // N_DP
    key_cols = KEY_VALUE_HEADS * HEAD_WIDTH // N_DP
    total = jnp.zeros((SEQUENCE_TOKENS, D), jnp.float32)
    for group_index in range(N_DP):
        q_lo = group_index * query_cols
        k_lo = group_index * key_cols
        head_part = jnp.dot(grad_q[:, q_lo:q_lo + query_cols], w_query[q_lo:q_lo + query_cols], preferred_element_type=jnp.float32)
        head_part = head_part + jnp.dot(grad_k[:, k_lo:k_lo + key_cols], w_key[k_lo:k_lo + key_cols], preferred_element_type=jnp.float32)
        head_part = head_part + jnp.dot(gradient_values[:, k_lo:k_lo + key_cols], w_value[k_lo:k_lo + key_cols], preferred_element_type=jnp.float32)
        rounded = lax.optimization_barrier(head_part.astype(jnp.bfloat16))
        total = total + rounded.astype(jnp.float32)
    d_inputs = total.astype(jnp.bfloat16)
    grad_wq = jnp.dot(grad_q.T, inputs, preferred_element_type=jnp.float32)
    grad_wk = jnp.dot(grad_k.T, inputs, preferred_element_type=jnp.float32)
    grad_wv = jnp.dot(gradient_values.T, inputs, preferred_element_type=jnp.float32)
    return (d_inputs, grad_wq, grad_wk, grad_wv)
```

```python
import functools

import jax
import jax.numpy as jnp
import numpy as np
from jax import lax
from jax.experimental import pallas as pl
from jax.experimental.pallas import tpu as pltpu
from jax.sharding import Mesh
from jax.sharding import PartitionSpec as P

HEAD_WIDTH = 64
GRID_W = 64
GROUP = 2
LANES = 128
MESH = pl.DeviceIdType.MESH
F32 = jnp.float32
BF16 = jnp.bfloat16

norm_eps = 1e-06
axial_base = 10000.0

NT = (((1,), (1,)), ((), ()))
NN = (((1,), (0,)), ((), ()))
TN = (((0,), (0,)), ((), ()))


def dot(a, b, dims):
    return lax.dot_general(a, b, dims, preferred_element_type=F32)


def rotation_constants(grid_rows):
    quarter = HEAD_WIDTH // 4
    freqs = axial_base ** (-np.arange(quarter, dtype=np.float64) / quarter)
    by_row = np.arange(grid_rows, dtype=np.float64)[:, None] * freqs
    by_col = np.arange(GRID_W, dtype=np.float64)[:, None] * freqs

    def wide(first, second):
        head = np.concatenate([first, first, second, second], axis=1)
        return np.concatenate([head, head], axis=1)

    none_r, none_c = np.zeros_like(by_row), np.zeros_like(by_col)
    rows = np.stack([wide(np.cos(by_row), none_r), wide(np.sin(by_row), none_r)])
    cols = np.stack([wide(none_c, np.cos(by_col)), wide(none_c, np.sin(by_col))])
    return rows.astype(np.float32), cols.astype(np.float32)


def farthest_first(n):
    return sorted(range(1, n), key=lambda d: -min(d, n - d))


def nearest_first(n):
    return sorted(range(1, n), key=lambda d: min(d, n - d))


def kernel(
    sizes, x_ref, wq_ref, wk_ref, wv_ref, qg_ref, kg_ref, do_ref, rows_ref, cols_ref,
    din_ref, gw_ref,
    w_all, x_buf, kv_buf, q_buf, do_buf, qa, doa, e_buf, dp_buf, stat, cfac, delta, st_buf,
    dqt, dq_all, dkv_send, dkv_buf, dq_send, dq_buf, g_buf, xin, hp_send, hp_buf, gw_part, gwr_buf,
    load_sem, kv_ss, kv_rs, q_ss, q_rs, do_ss, do_rs, st_ss, st_rs, xin_ss, xin_rs, dkv_ss, dkv_rs,
    dq_ss, dq_rs, g_ss, g_rs, hp_ss, hp_rs, gwr_ss, gwr_rs, agz_ss, agz_rs, agx_ss, agx_rs,
):
    Z, X, Y, C, T, D, R, CH = sizes
    DX = D // X
    DC = D // (Y * C)
    WR = w_all.shape[0]
    PZ = WR // Z
    z, x, y, c = (lax.axis_index(a) for a in ("z", "x", "y", "c"))

    def on_z(d):
        return {"z": lax.rem(z + d, Z)}

    def on_x(d):
        return {"x": lax.rem(x + d, X)}

    def on_dp(dy, dc):
        return {"y": lax.rem(y + dy, Y), "c": lax.rem(c + dc, C)}

    def remote(src, dst, ss, rs, dev):
        return pltpu.make_async_remote_copy(
            src_ref=src, dst_ref=dst, send_sem=ss, recv_sem=rs, device_id=dev, device_id_type=MESH
        )

    dp_pairs = [(dy, dc) for dy in [0] + nearest_first(Y) for dc in range(C) if (dy, dc) != (0, 0)]

    nq, nk = wq_ref.shape[0], wk_ref.shape[0]
    loads = [
        pltpu.make_async_copy(x_ref, x_buf, load_sem.at[0]),
        pltpu.make_async_copy(wq_ref, w_all.at[pl.ds(0, nq)], load_sem.at[1]),
        pltpu.make_async_copy(wk_ref, w_all.at[pl.ds(nq, nk)], load_sem.at[2]),
        pltpu.make_async_copy(wv_ref, w_all.at[pl.ds(nq + nk, nk)], load_sem.at[3]),
        pltpu.make_async_copy(do_ref, do_buf.at[x], load_sem.at[4]),
    ]
    for load in loads:
        load.start()
    barrier = pltpu.get_barrier_semaphore()
    for d in range(1, Z):
        pl.semaphore_signal(barrier, inc=1, device_id=on_z(d), device_id_type=MESH)
    for d in range(1, X):
        pl.semaphore_signal(barrier, inc=1, device_id=on_x(d), device_id_type=MESH)
    for dy, dc in dp_pairs:
        pl.semaphore_signal(barrier, inc=1, device_id=on_dp(dy, dc), device_id_type=MESH)

    lane = lax.broadcasted_iota(jnp.int32, (T, LANES), 1)
    low = lax.rem(lane, 32) < 16
    head0 = lane < HEAD_WIDTH
    n_rows = T // GRID_W
    first_row = (z * X + x) * n_rows

    def table(k):
        return jnp.concatenate(
            [rows_ref[k, pl.ds(first_row + j, 1), :] + cols_ref[k] for j in range(n_rows)], axis=0
        )

    cos = table(0)
    sin = table(1)
    sin = jnp.where(low, -sin, sin)

    def turned(v):
        return jnp.where(low, pltpu.roll(v, LANES - 16, 1), pltpu.roll(v, 16, 1))

    def rotate(v):
        return v * cos + turned(v) * sin

    def rotate_back(v):
        return v * cos - turned(v) * sin

    def head_mean(v):
        first = jnp.sum(jnp.where(head0, v, 0.0), axis=1, keepdims=True)
        second = jnp.sum(jnp.where(head0, 0.0, v), axis=1, keepdims=True)
        return jnp.where(head0, first, second) * (1.0 / HEAD_WIDTH)

    qg = jnp.concatenate([qg_ref[...], qg_ref[...]], axis=1)
    kg = jnp.concatenate([kg_ref[...], kg_ref[...]], axis=1)

    for load in loads:
        load.wait()
    raw = dot(x_buf[...], w_all[...], NT).astype(BF16).astype(F32)
    q_raw = raw[:, :LANES]
    kv_raw = raw[:, LANES:]
    q_inv = lax.rsqrt(head_mean(q_raw * q_raw) + norm_eps)
    q_hat = q_raw * q_inv
    k_inv = lax.rsqrt(head_mean(kv_raw * kv_raw) + norm_eps)
    k_hat = kv_raw * k_inv
    q_buf[x] = rotate(q_hat * qg).astype(BF16)
    kv_buf[0] = jnp.where(head0, rotate(k_hat * kg), kv_raw).astype(BF16)

    pl.semaphore_wait(barrier, (Z - 1) + (X - 1) + len(dp_pairs))

    kv_copies, q_copies, do_copies = {}, {}, {}
    for d in nearest_first(Z):
        kv_copies[d] = remote(kv_buf.at[0], kv_buf.at[d], kv_ss.at[d], kv_rs.at[d], on_z(d))
        kv_copies[d].start()
    for d in nearest_first(X):
        q_copies[d] = remote(q_buf.at[x], q_buf.at[x], q_ss.at[d], q_rs.at[d], on_x(d))
        q_copies[d].start()
        do_copies[d] = remote(do_buf.at[x], do_buf.at[x], do_ss.at[d], do_rs.at[d], on_x(d))
        do_copies[d].start()
    for d in range(1, X):
        q_copies[d].wait()
        do_copies[d].wait()

    q_rows = q_buf[...].reshape(X * T, LANES).astype(F32) * (HEAD_WIDTH**-0.5)
    do_rows = do_buf[...].reshape(X * T, LANES).astype(F32)
    keep = lax.broadcasted_iota(jnp.int32, (X * T, LANES), 1) < HEAD_WIDTH
    half = R // GROUP
    qa[0:half] = jnp.where(keep, q_rows, 0.0).astype(BF16).reshape(half, CH, LANES)
    qa[half:] = (
        jnp.where(keep, pltpu.roll(q_rows, HEAD_WIDTH, 1), 0.0).astype(BF16).reshape(half, CH, LANES)
    )
    doa[0:half] = (
        jnp.where(keep, 0.0, pltpu.roll(do_rows, HEAD_WIDTH, 1)).astype(BF16).reshape(half, CH, LANES)
    )
    doa[half:] = jnp.where(keep, 0.0, do_rows).astype(BF16).reshape(half, CH, LANES)

    for d in [0] + nearest_first(Z):
        if d:
            kv_copies[d].wait()

        def forward(r, carry, d=d):
            kv = kv_buf[d]
            s = dot(kv, qa[r], NT)
            dp = dot(kv, doa[r], NT)
            m = jnp.max(s, axis=0, keepdims=True)
            e = jnp.exp(s - m)
            stat[d, 0, r] = m
            stat[d, 1, r] = jnp.sum(e, axis=0, keepdims=True)
            stat[d, 2, r] = jnp.sum(e * dp, axis=0, keepdims=True)
            e_buf[d, r] = e
            dp_buf[d, r] = dp
            return carry

        lax.fori_loop(0, R, forward, 0)

    top = stat[0, 0]
    for d in range(1, Z):
        top = jnp.maximum(top, stat[d, 0])
    total = jnp.zeros_like(top)
    weighted = jnp.zeros_like(top)
    for d in range(Z):
        f = jnp.exp(stat[d, 0] - top)
        total = total + stat[d, 1] * f
        weighted = weighted + stat[d, 2] * f
    st_buf[0, 0] = top
    st_buf[0, 1] = total
    st_buf[0, 2] = weighted
    st_copies = {}
    for d in nearest_first(X):
        st_copies[d] = remote(st_buf.at[0], st_buf.at[d], st_ss.at[d], st_rs.at[d], on_x(d))
        st_copies[d].start()
    xin_copies = {}
    for d in nearest_first(X):
        cols = pl.multiple_of(lax.rem(x + d, X) * DX, LANES)
        xin_copies[d] = remote(
            x_buf.at[:, pl.ds(cols, DX)], xin.at[d], xin_ss.at[d], xin_rs.at[d], on_x(d)
        )
        xin_copies[d].start()
    for d in range(1, X):
        st_copies[d].wait()
    top = st_buf[0, 0]
    for d in range(1, X):
        top = jnp.maximum(top, st_buf[d, 0])
    total = jnp.zeros_like(top)
    weighted = jnp.zeros_like(top)
    for d in range(X):
        f = jnp.exp(st_buf[d, 0] - top)
        total = total + st_buf[d, 1] * f
        weighted = weighted + st_buf[d, 2] * f
    log_total = top + jnp.log(total)
    delta[...] = weighted / total
    for d in range(Z):
        cfac[d] = jnp.exp(stat[d, 0] - log_total)

    dqt[...] = jnp.zeros_like(dqt)
    dkv_copies = {}
    dkv_own = None
    for d in farthest_first(Z) + [0]:
        k_t = kv_buf[d].astype(F32).T[:HEAD_WIDTH].astype(BF16)

        def backward(r, acc, d=d, k_t=k_t):
            p = e_buf[d, r] * cfac[d, r]
            ds = (p * (dp_buf[d, r] - delta[r])).astype(BF16)
            acc = acc + dot(p.astype(BF16), doa[r], NN) + dot(ds, qa[r], NN)
            dqt[r] += dot(k_t, ds, NN)
            return acc

        acc = lax.fori_loop(0, R, backward, jnp.zeros((T, LANES), F32))
        if d:
            dkv_send[d] = acc.astype(BF16)
            dkv_copies[d] = remote(
                dkv_send.at[d], dkv_buf.at[d], dkv_ss.at[d], dkv_rs.at[d], on_z(Z - d)
            )
            dkv_copies[d].start()
        else:
            dkv_own = acc

    dq_rows = jnp.concatenate(
        [jnp.concatenate([dqt[r], dqt[half + r]], axis=0).T for r in range(half)], axis=0
    )
    dq_all[...] = dq_rows.reshape(X, T, LANES)
    dq_send[...] = dq_rows.astype(BF16).reshape(X, T, LANES)
    dq_copies = {}
    for d in range(1, X):
        dq_copies[d] = remote(
            dq_send.at[lax.rem(x + X - d, X)], dq_buf.at[d], dq_ss.at[d], dq_rs.at[d], on_x(X - d)
        )
        dq_copies[d].start()
    dq_own = dq_all[x]
    for d in range(1, X):
        dq_copies[d].wait()
        dq_own = dq_own + dq_buf[d].astype(F32)
    for d in range(1, Z):
        dkv_copies[d].wait()
        dkv_own = dkv_own + dkv_buf[d].astype(F32)

    def norm_back(grads, normed, inv, gain):
        u = rotate_back(grads) * gain
        return inv * (u - normed * head_mean(u * normed))

    grad_q = norm_back(dq_own * (HEAD_WIDTH**-0.5), q_hat, q_inv, qg)
    grad_k = norm_back(jnp.where(head0, dkv_own, 0.0), k_hat, k_inv, kg)
    grad_kv = jnp.where(head0, grad_k, dkv_own)
    g = jnp.concatenate([grad_q.astype(BF16), grad_kv.astype(BF16)], axis=1)
    g_buf[0] = g
    g_copies = {}
    for d in nearest_first(X):
        g_copies[d] = remote(g_buf.at[0], g_buf.at[d], g_ss.at[d], g_rs.at[d], on_x(d))
        g_copies[d].start()

    def part_for(dy, dc):
        j = lax.rem(y + dy, Y) * C + lax.rem(c + dc, C)
        return dot(g, w_all[:, pl.ds(pl.multiple_of(j * DC, LANES), DC)], NN).astype(BF16)

    hp_copies = {}
    for dy, dc in reversed(dp_pairs):
        slot = dy * C + dc
        hp_send[slot] = part_for(dy, dc)
        hp_copies[slot] = remote(
            hp_send.at[slot], hp_buf.at[slot], hp_ss.at[slot], hp_rs.at[slot], on_dp(dy, dc)
        )
        hp_copies[slot].start()
    din = part_for(0, 0).astype(F32)

    cols = pl.multiple_of(x * DX, LANES)
    gw = dot(g, x_buf[:, pl.ds(cols, DX)], TN)
    for d in range(1, X):
        g_copies[d].wait()
        xin_copies[d].wait()
        gw = gw + dot(g_buf[d], xin[d], TN)
    gw_part[...] = gw.astype(BF16)
    gwr_copies = {}
    for d in farthest_first(Z):
        rows = pl.multiple_of(lax.rem(z + d, Z) * PZ, PZ)
        gwr_copies[d] = remote(
            gw_part.at[pl.ds(rows, PZ)], gwr_buf.at[d], gwr_ss.at[d], gwr_rs.at[d], on_z(d)
        )
        gwr_copies[d].start()
    my_rows = pl.multiple_of(z * PZ, PZ)
    piece = gw_part[pl.ds(my_rows, PZ), :].astype(F32)
    for d in range(1, Z):
        gwr_copies[d].wait()
        piece = piece + gwr_buf[d].astype(F32)
    gw_ref[pl.ds(my_rows, PZ), pl.ds(cols, DX)] = piece.astype(BF16)

    def region(dz):
        rows = pl.multiple_of(lax.rem(z + Z - dz, Z) * PZ, PZ)
        return gw_ref.at[pl.ds(rows, PZ), pl.ds(cols, DX)]

    agz_copies, agx_copies = {}, {}
    own = region(0)
    for d in nearest_first(Z):
        agz_copies[d] = remote(own, own, agz_ss.at[d], agz_rs.at[d], on_z(d))
        agz_copies[d].start()
    for dz in [0] + nearest_first(Z):
        if dz:
            agz_copies[dz].wait_recv()
        block = region(dz)
        for d in nearest_first(X):
            agx_copies[dz, d] = remote(
                block, block, agx_ss.at[d, dz], agx_rs.at[d, dz], on_x(d)
            )
            agx_copies[dz, d].start()

    for slot, copy in hp_copies.items():
        copy.wait()
        din = din + hp_buf[slot].astype(F32)
    din_ref[...] = din.astype(BF16)
    for copy in agx_copies.values():
        copy.wait()
    for copy in agz_copies.values():
        copy.wait_send()


def make_body(Z, X, Y, C):
    def body(inputs, w_query, w_key, w_value, query_gain, key_gain, grad_out):
        T, D = inputs.shape
        nq, nk = w_query.shape[0], w_key.shape[0]
        per_head = X * T
        CH = 256 if per_head % 256 == 0 else 384
        R = GROUP * per_head // CH
        rows, cols = rotation_constants(Z * X * T // GRID_W)
        DX, DC, PZ = D // X, D // (Y * C), (nq + 2 * nk) // Z
        sizes = (Z, X, Y, C, T, D, R, CH)
        dma = pltpu.SemaphoreType.DMA
        pair = lambda *n: [dma(n), dma(n)]
        vmem = pl.BlockSpec(memory_space=pltpu.VMEM)
        hbm = pl.BlockSpec(memory_space=pl.ANY)
        din, gw = pl.pallas_call(
            functools.partial(kernel, sizes),
            out_shape=(
                jax.ShapeDtypeStruct((T, DC), BF16),
                jax.ShapeDtypeStruct((nq + 2 * nk, D), BF16),
            ),
            in_specs=[hbm, hbm, hbm, hbm, vmem, vmem, hbm, vmem, vmem],
            out_specs=(vmem, vmem),
            scratch_shapes=[
                pltpu.VMEM((nq + 2 * nk, D), BF16),
                pltpu.VMEM((T, D), BF16),
                pltpu.VMEM((Z, T, LANES), BF16),
                pltpu.VMEM((X, T, LANES), BF16),
                pltpu.VMEM((X, T, LANES), BF16),
                pltpu.VMEM((R, CH, LANES), BF16),
                pltpu.VMEM((R, CH, LANES), BF16),
                pltpu.VMEM((Z, R, T, CH), F32),
                pltpu.VMEM((Z, R, T, CH), F32),
                pltpu.VMEM((Z, 3, R, 1, CH), F32),
                pltpu.VMEM((Z, R, 1, CH), F32),
                pltpu.VMEM((R, 1, CH), F32),
                pltpu.VMEM((X, 3, R, 1, CH), F32),
                pltpu.VMEM((R, HEAD_WIDTH, CH), F32),
                pltpu.VMEM((X, T, LANES), F32),
                pltpu.VMEM((Z, T, LANES), BF16),
                pltpu.VMEM((Z, T, LANES), BF16),
                pltpu.VMEM((X, T, LANES), BF16),
                pltpu.VMEM((X, T, LANES), BF16),
                pltpu.VMEM((X, T, nq + 2 * nk), BF16),
                pltpu.VMEM((X, T, DX), BF16),
                pltpu.VMEM((Y * C, T, DC), BF16),
                pltpu.VMEM((Y * C, T, DC), BF16),
                pltpu.VMEM((nq + 2 * nk, DX), BF16),
                pltpu.VMEM((Z, PZ, DX), BF16),
                dma((5,)),
                *pair(Z), *pair(X), *pair(X), *pair(X), *pair(X), *pair(Z),
                *pair(X), *pair(X), *pair(Y * C), *pair(Z), *pair(Z), *pair(X, Z),
            ],
            compiler_params=pltpu.CompilerParams(
                collective_id=0, has_side_effects=True, vmem_limit_bytes=60 * 1024 * 1024
            ),
            name="attention_backward",
        )(
            inputs, w_query, w_key, w_value, query_gain.reshape(1, -1), key_gain.reshape(1, -1),
            grad_out, jnp.asarray(rows), jnp.asarray(cols),
        )
        gw = gw.astype(F32)
        return din, gw[:nq], gw[nq : nq + nk], gw[nq + nk :]

    return body


def solution(mesh):
    Z, X, Y, C = 8, 4, mesh.shape["dp"] // 2, 2
    finer = Mesh(mesh.devices.reshape(Z, X, Y, C), ("z", "x", "y", "c"))
    sp, dp = ("z", "x"), ("y", "c")
    return jax.shard_map(
        make_body(Z, X, Y, C),
        mesh=finer,
        in_specs=(P(sp, None), P(dp, None), P(dp, None), P(dp, None), P(), P(), P(sp, dp)),
        out_specs=(P(sp, dp), P(dp, None), P(dp, None), P(dp, None)),
        check_vma=False,
    )
```

```python
import functools

import jax
import jax.numpy as jnp
import numpy as np
from jax import lax
from jax.experimental import pallas as pl
from jax.experimental.pallas import tpu as pltpu
from jax.sharding import Mesh
from jax.sharding import PartitionSpec as P

HEAD_WIDTH = 64
GRID_W = 64
GROUP = 2
LANES = 128
MESH = pl.DeviceIdType.MESH
F32 = jnp.float32
BF16 = jnp.bfloat16

norm_eps = 1e-06
axial_base = 10000.0

NT = (((1,), (1,)), ((), ()))
NN = (((1,), (0,)), ((), ()))
TN = (((0,), (0,)), ((), ()))


def dot(a, b, dims):
    return lax.dot_general(a, b, dims, preferred_element_type=F32)


def mark(name):
    pass


def rotation_constants(grid_rows):
    quarter = HEAD_WIDTH // 4
    freqs = axial_base ** (-np.arange(quarter, dtype=np.float64) / quarter)
    by_row = np.arange(grid_rows, dtype=np.float64)[:, None] * freqs
    by_col = np.arange(GRID_W, dtype=np.float64)[:, None] * freqs

    def wide(first, second):
        head = np.concatenate([first, first, second, second], axis=1)
        return np.concatenate([head, head], axis=1)

    none_r, none_c = np.zeros_like(by_row), np.zeros_like(by_col)
    rows = np.stack([wide(np.cos(by_row), none_r), wide(np.sin(by_row), none_r)])
    cols = np.stack([wide(none_c, np.cos(by_col)), wide(none_c, np.sin(by_col))])
    return rows.astype(np.float32), cols.astype(np.float32)


def farthest_first(n):
    return sorted(range(1, n), key=lambda d: -min(d, n - d))


def nearest_first(n):
    return sorted(range(1, n), key=lambda d: min(d, n - d))


def kernel(
    sizes, x_ref, wq_ref, wk_ref, wv_ref, qg_ref, kg_ref, do_ref, rows_ref, cols_ref,
    din_ref, gw_ref,
    w_all, x_buf, kv_buf, q_buf, do_buf, w_buf, e_buf, dp_buf, stat, cfac, delta, st_buf,
    dqt, dkv_send, dkv_buf, dq_send, dq_buf, g_buf, xin, hp_send, hp_buf, gw_part, gwr_buf,
    load_sem, kv_ss, kv_rs, q_ss, q_rs, do_ss, do_rs, st_ss, st_rs, xin_ss, xin_rs, dkv_ss, dkv_rs,
    dq_ss, dq_rs, g_ss, g_rs, hp_ss, hp_rs, gwr_ss, gwr_rs, agz_ss, agz_rs, agx_ss, agx_rs,
):
    Z, X, Y, C, T, D = sizes
    tiles = GROUP * T // LANES
    DX = D // X
    DC = D // (Y * C)
    WR = w_all.shape[0]
    PZ = WR // Z
    z, x, y, c = (lax.axis_index(a) for a in ("z", "x", "y", "c"))

    def on_z(d):
        return {"z": lax.rem(z + d, Z)}

    def on_x(d):
        return {"x": lax.rem(x + d, X)}

    def on_dp(dy, dc):
        return {"y": lax.rem(y + dy, Y), "c": lax.rem(c + dc, C)}

    def remote(src, dst, ss, rs, dev):
        return pltpu.make_async_remote_copy(
            src_ref=src, dst_ref=dst, send_sem=ss, recv_sem=rs, device_id=dev, device_id_type=MESH
        )

    dp_pairs = [(dy, dc) for dy in [0] + nearest_first(Y) for dc in range(C) if (dy, dc) != (0, 0)]

    nq, nk = wq_ref.shape[0], wk_ref.shape[0]
    loads = [
        pltpu.make_async_copy(x_ref, x_buf, load_sem.at[0]),
        pltpu.make_async_copy(wq_ref, w_all.at[pl.ds(0, nq)], load_sem.at[1]),
        pltpu.make_async_copy(wk_ref, w_all.at[pl.ds(nq, nk)], load_sem.at[2]),
        pltpu.make_async_copy(wv_ref, w_all.at[pl.ds(nq + nk, nk)], load_sem.at[3]),
        pltpu.make_async_copy(do_ref, do_buf.at[0], load_sem.at[4]),
    ]
    mark("a_issue_loads")
    for load in loads:
        load.start()
    barrier = pltpu.get_barrier_semaphore()
    for d in range(1, Z):
        pl.semaphore_signal(barrier, inc=1, device_id=on_z(d), device_id_type=MESH)
    for d in range(1, X):
        pl.semaphore_signal(barrier, inc=1, device_id=on_x(d), device_id_type=MESH)
    for dy, dc in dp_pairs:
        pl.semaphore_signal(barrier, inc=1, device_id=on_dp(dy, dc), device_id_type=MESH)

    lane = lax.broadcasted_iota(jnp.int32, (T, LANES), 1)
    low = lax.rem(lane, 32) < 16
    head0 = lane < HEAD_WIDTH
    n_rows = T // GRID_W
    first_row = (z * X + x) * n_rows

    def table(k):
        return jnp.concatenate(
            [rows_ref[k, pl.ds(first_row + j, 1), :] + cols_ref[k] for j in range(n_rows)], axis=0
        )

    cos = table(0)
    sin = table(1)
    sin = jnp.where(low, -sin, sin)

    def turned(v):
        return jnp.where(low, pltpu.roll(v, LANES - 16, 1), pltpu.roll(v, 16, 1))

    def rotate(v):
        return v * cos + turned(v) * sin

    def rotate_back(v):
        return v * cos - turned(v) * sin

    def head_mean(v):
        first = jnp.sum(jnp.where(head0, v, 0.0), axis=1, keepdims=True)
        second = jnp.sum(jnp.where(head0, 0.0, v), axis=1, keepdims=True)
        return jnp.where(head0, first, second) * (1.0 / HEAD_WIDTH)

    mark("b_proj")
    qg = jnp.concatenate([qg_ref[...], qg_ref[...]], axis=1)
    kg = jnp.concatenate([kg_ref[...], kg_ref[...]], axis=1)

    for load in loads:
        load.wait()
    raw = dot(x_buf[...], w_all[...], NT).astype(BF16).astype(F32)
    q_raw = raw[:, :LANES]
    kv_raw = raw[:, LANES:]
    q_inv = lax.rsqrt(head_mean(q_raw * q_raw) + norm_eps)
    q_hat = q_raw * q_inv
    k_inv = lax.rsqrt(head_mean(kv_raw * kv_raw) + norm_eps)
    k_hat = kv_raw * k_inv
    q_buf[0] = rotate(q_hat * qg).astype(BF16)
    kv_buf[0] = jnp.where(head0, rotate(k_hat * kg), kv_raw).astype(BF16)

    mark("c_barrier")
    pl.semaphore_wait(barrier, (Z - 1) + (X - 1) + len(dp_pairs))

    mark("d_issue")
    kv_copies, q_copies, do_copies = {}, {}, {}
    for d in nearest_first(Z):
        kv_copies[d] = remote(kv_buf.at[0], kv_buf.at[d], kv_ss.at[d], kv_rs.at[d], on_z(d))
        kv_copies[d].start()
    for d in nearest_first(X):
        q_copies[d] = remote(q_buf.at[0], q_buf.at[d], q_ss.at[d], q_rs.at[d], on_x(d))
        q_copies[d].start()
        do_copies[d] = remote(do_buf.at[0], do_buf.at[d], do_ss.at[d], do_rs.at[d], on_x(d))
        do_copies[d].start()

    def src_x(d):
        return lax.rem(x + X - d, X)

    def take_queries(d):
        if d:
            mark(f"e_qwait{d}")
            q_copies[d].wait()
            do_copies[d].wait()
        mark(f"f_build{d}")
        q_rows = q_buf[d].astype(F32) * (HEAD_WIDTH**-0.5)
        do_rows = do_buf[d].astype(F32)
        qa = jnp.concatenate(
            [jnp.where(head0, q_rows, 0.0), jnp.where(head0, pltpu.roll(q_rows, HEAD_WIDTH, 1), 0.0)], axis=0
        ).astype(BF16)
        doa = jnp.concatenate(
            [jnp.where(head0, 0.0, pltpu.roll(do_rows, HEAD_WIDTH, 1)), jnp.where(head0, 0.0, do_rows)], axis=0
        ).astype(BF16)
        for t in range(tiles):
            w_buf[d, t, 0:LANES] = qa[t * LANES : (t + 1) * LANES]
            w_buf[d, t, LANES:] = doa[t * LANES : (t + 1) * LANES]

    def take_keys(d):
        if d:
            mark(f"g_kvwait{d}")
            kv_copies[d].wait()

    def forward(d, q):
        kv = kv_buf[d]
        for t in range(tiles):
            both = dot(kv, w_buf[q, t], NT)
            s = both[:, :LANES]
            dp = both[:, LANES:]
            m = jnp.max(s, axis=0, keepdims=True)
            e = jnp.exp(s - m)
            stat[d, q, t, 0] = m
            stat[d, q, t, 1] = jnp.sum(e, axis=0, keepdims=True)
            stat[d, q, t, 2] = jnp.sum(e * dp, axis=0, keepdims=True)
            e_buf[d, q, t] = e
            dp_buf[d, q, t] = dp

    arrivals = []
    zs, xs = [0] + nearest_first(Z), [0] + nearest_first(X)
    order = [("k", 0, 0.0), ("q", 0, 0.0)]
    order += [("k", d, 1.0 + 2.0 * min(d, Z - d) - (d < Z - d) * 0.1) for d in zs[1:]]
    order += [("q", d, 3.5 + 3.0 * (min(d, X - d) - 1) - (d < X - d) * 0.1) for d in xs[1:]]
    keys_in, queries_in = [], []
    for kind, d, _ in sorted(order, key=lambda item: item[2]):
        if kind == "k":
            take_keys(d)
            keys_in.append(d)
            blocks = [(d, q) for q in queries_in]
        else:
            take_queries(d)
            queries_in.append(d)
            blocks = [(k, d) for k in keys_in]
        if blocks:
            mark(f"h_fwd_{kind}{d}")
        for k, q in blocks:
            forward(k, q)

    def merged(parts):
        top = parts[0][0]
        for m, _, _ in parts[1:]:
            top = jnp.maximum(top, m)
        total, weighted = jnp.zeros_like(top), jnp.zeros_like(top)
        for m, l, w in parts:
            f = jnp.exp(m - top)
            total = total + l * f
            weighted = weighted + w * f
        return top, total, weighted

    mark("i_stat")
    for q in range(X):
        parts = [[stat[d, q, :, i] for i in range(3)] for d in range(Z)]
        for i, value in enumerate(merged(parts)):
            st_buf[0, src_x(q), i] = value
    st_copies = {}
    for d in nearest_first(X):
        st_copies[d] = remote(st_buf.at[0], st_buf.at[d], st_ss.at[d], st_rs.at[d], on_x(d))
        st_copies[d].start()
    xin_copies = {}
    for d in nearest_first(X):
        cols = pl.multiple_of(lax.rem(x + d, X) * DX, LANES)
        xin_copies[d] = remote(
            x_buf.at[:, pl.ds(cols, DX)], xin.at[d], xin_ss.at[d], xin_rs.at[d], on_x(d)
        )
        xin_copies[d].start()
    mark("j_stwait")
    for d in range(1, X):
        st_copies[d].wait()
    mark("k_comb")
    for q in range(X):
        at = src_x(q)
        top, total, weighted = merged([[st_buf[d, at, i] for i in range(3)] for d in range(X)])
        log_total = top + jnp.log(total)
        delta[q] = weighted / total
        for d in range(Z):
            cfac[d, q] = jnp.exp(stat[d, q, :, 0] - log_total)

    dqt[...] = jnp.zeros_like(dqt)
    dkv_copies = {}
    dkv_own = None
    for d in farthest_first(Z) + [0]:
        mark(f"l_bwd{d}")
        k_t = kv_buf[d].astype(F32).T[:HEAD_WIDTH].astype(BF16)

        acc = jnp.zeros((T, LANES), F32)
        for q in range(X):
            scores_grad = []
            for t in range(tiles):
                p = e_buf[d, q, t] * cfac[d, q, t]
                ds = (p * (dp_buf[d, q, t] - delta[q, t])).astype(BF16)
                scores_grad.append(ds)
                acc = acc + dot(jnp.concatenate([ds, p.astype(BF16)], axis=1), w_buf[q, t], NN)
            dqt[q] += dot(k_t, jnp.concatenate(scores_grad, axis=1), NN)
        if d:
            dkv_send[d] = acc.astype(BF16)
            dkv_copies[d] = remote(
                dkv_send.at[d], dkv_buf.at[d], dkv_ss.at[d], dkv_rs.at[d], on_z(Z - d)
            )
            dkv_copies[d].start()
        else:
            dkv_own = acc

    mark("m_dq")
    dq_copies = {}

    def dq_of(q):
        rows = dqt[q].T
        return jnp.concatenate([rows[:T], rows[T:]], axis=1)

    for d in nearest_first(X):
        dq_send[d] = dq_of(d).astype(BF16)
        dq_copies[d] = remote(
            dq_send.at[d], dq_buf.at[d], dq_ss.at[d], dq_rs.at[d], on_x(X - d)
        )
        dq_copies[d].start()
    dq_own = dq_of(0)
    mark("n_dqwait")
    for d in range(1, X):
        dq_copies[d].wait()
        dq_own = dq_own + dq_buf[d].astype(F32)
    mark("o_dkvwait")
    for d in range(1, Z):
        dkv_copies[d].wait()
        dkv_own = dkv_own + dkv_buf[d].astype(F32)

    def norm_back(grads, normed, inv, gain):
        u = rotate_back(grads) * gain
        return inv * (u - normed * head_mean(u * normed))

    mark("p_normback")
    grad_q = norm_back(dq_own * (HEAD_WIDTH**-0.5), q_hat, q_inv, qg)
    grad_k = norm_back(jnp.where(head0, dkv_own, 0.0), k_hat, k_inv, kg)
    grad_kv = jnp.where(head0, grad_k, dkv_own)
    g = jnp.concatenate([grad_q.astype(BF16), grad_kv.astype(BF16)], axis=1)
    g_buf[0] = g
    g_copies = {}
    for d in nearest_first(X):
        g_copies[d] = remote(g_buf.at[0], g_buf.at[d], g_ss.at[d], g_rs.at[d], on_x(d))
        g_copies[d].start()

    def part_for(dy, dc):
        j = lax.rem(y + dy, Y) * C + lax.rem(c + dc, C)
        return dot(g, w_all[:, pl.ds(pl.multiple_of(j * DC, LANES), DC)], NN).astype(BF16)

    mark("q_hp")
    hp_copies = {}
    for dy, dc in reversed(dp_pairs):
        slot = dy * C + dc
        hp_send[slot] = part_for(dy, dc)
        hp_copies[slot] = remote(
            hp_send.at[slot], hp_buf.at[slot], hp_ss.at[slot], hp_rs.at[slot], on_dp(dy, dc)
        )
        hp_copies[slot].start()
    din = part_for(0, 0).astype(F32)

    mark("r_gw")
    cols = pl.multiple_of(x * DX, LANES)
    gw = dot(g, x_buf[:, pl.ds(cols, DX)], TN)
    for d in range(1, X):
        g_copies[d].wait()
        xin_copies[d].wait()
        gw = gw + dot(g_buf[d], xin[d], TN)
    gw_part[...] = gw.astype(BF16)
    gwr_copies = {}
    for d in farthest_first(Z):
        rows = pl.multiple_of(lax.rem(z + d, Z) * PZ, PZ)
        gwr_copies[d] = remote(
            gw_part.at[pl.ds(rows, PZ)], gwr_buf.at[d], gwr_ss.at[d], gwr_rs.at[d], on_z(d)
        )
        gwr_copies[d].start()
    mark("s_gwrwait")
    my_rows = pl.multiple_of(z * PZ, PZ)
    piece = gw_part[pl.ds(my_rows, PZ), :].astype(F32)
    for d in range(1, Z):
        gwr_copies[d].wait()
        piece = piece + gwr_buf[d].astype(F32)
    gw_ref[pl.ds(my_rows, PZ), pl.ds(cols, DX)] = piece.astype(BF16)

    def region(dz):
        rows = pl.multiple_of(lax.rem(z + Z - dz, Z) * PZ, PZ)
        return gw_ref.at[pl.ds(rows, PZ), pl.ds(cols, DX)]

    mark("t_agz")
    agz_copies, agx_copies = {}, {}
    own = region(0)
    for d in nearest_first(Z):
        agz_copies[d] = remote(own, own, agz_ss.at[d], agz_rs.at[d], on_z(d))
        agz_copies[d].start()
    for dz in [0] + nearest_first(Z):
        if dz:
            agz_copies[dz].wait_recv()
        block = region(dz)
        for d in nearest_first(X):
            agx_copies[dz, d] = remote(
                block, block, agx_ss.at[d, dz], agx_rs.at[d, dz], on_x(d)
            )
            agx_copies[dz, d].start()

    mark("u_hpwait")
    for slot, copy in hp_copies.items():
        copy.wait()
        din = din + hp_buf[slot].astype(F32)
    din_ref[...] = din.astype(BF16)
    mark("v_agxwait")
    for copy in agx_copies.values():
        copy.wait()
    for copy in agz_copies.values():
        copy.wait_send()
    mark(None)


def widen(gw_ref, *out_refs):
    first = 0
    for ref in out_refs:
        ref[...] = gw_ref[first : first + ref.shape[0]].astype(F32)
        first += ref.shape[0]


def make_body(Z, X, Y, C):
    def body(inputs, w_query, w_key, w_value, query_gain, key_gain, grad_out):
        T, D = inputs.shape
        nq, nk = w_query.shape[0], w_key.shape[0]
        rows, cols = rotation_constants(Z * X * T // GRID_W)
        DX, DC, PZ = D // X, D // (Y * C), (nq + 2 * nk) // Z
        sizes = (Z, X, Y, C, T, D)
        tiles = GROUP * T // LANES
        dma = pltpu.SemaphoreType.DMA
        pair = lambda *n: [dma(n), dma(n)]
        vmem = pl.BlockSpec(memory_space=pltpu.VMEM)
        hbm = pl.BlockSpec(memory_space=pl.ANY)
        din, gw = pl.pallas_call(
            functools.partial(kernel, sizes),
            out_shape=(
                jax.ShapeDtypeStruct((T, DC), BF16),
                jax.ShapeDtypeStruct((nq + 2 * nk, D), BF16),
            ),
            in_specs=[hbm, hbm, hbm, hbm, vmem, vmem, hbm, vmem, vmem],
            out_specs=(vmem, vmem),
            scratch_shapes=[
                pltpu.VMEM((nq + 2 * nk, D), BF16),
                pltpu.VMEM((T, D), BF16),
                pltpu.VMEM((Z, T, LANES), BF16),
                pltpu.VMEM((X, T, LANES), BF16),
                pltpu.VMEM((X, T, LANES), BF16),
                pltpu.VMEM((X, tiles, 2 * LANES, LANES), BF16),
                pltpu.VMEM((Z, X, tiles, T, LANES), F32),
                pltpu.VMEM((Z, X, tiles, T, LANES), F32),
                pltpu.VMEM((Z, X, tiles, 3, 1, LANES), F32),
                pltpu.VMEM((Z, X, tiles, 1, LANES), F32),
                pltpu.VMEM((X, tiles, 1, LANES), F32),
                pltpu.VMEM((X, X, 3, tiles, 1, LANES), F32),
                pltpu.VMEM((X, HEAD_WIDTH, GROUP * T), F32),
                pltpu.VMEM((Z, T, LANES), BF16),
                pltpu.VMEM((Z, T, LANES), BF16),
                pltpu.VMEM((X, T, LANES), BF16),
                pltpu.VMEM((X, T, LANES), BF16),
                pltpu.VMEM((X, T, nq + 2 * nk), BF16),
                pltpu.VMEM((X, T, DX), BF16),
                pltpu.VMEM((Y * C, T, DC), BF16),
                pltpu.VMEM((Y * C, T, DC), BF16),
                pltpu.VMEM((nq + 2 * nk, DX), BF16),
                pltpu.VMEM((Z, PZ, DX), BF16),
                dma((5,)),
                *pair(Z), *pair(X), *pair(X), *pair(X), *pair(X), *pair(Z),
                *pair(X), *pair(X), *pair(Y * C), *pair(Z), *pair(Z), *pair(X, Z),
            ],
            compiler_params=pltpu.CompilerParams(
                collective_id=0, has_side_effects=True, vmem_limit_bytes=60 * 1024 * 1024
            ),
            name="attention_backward",
        )(
            inputs, w_query, w_key, w_value, query_gain.reshape(1, -1), key_gain.reshape(1, -1),
            grad_out, jnp.asarray(rows), jnp.asarray(cols),
        )
        widened = [jax.ShapeDtypeStruct((n, D), F32) for n in (nq, nk, nk)]
        strip = D // 2
        return din, *pl.pallas_call(
            widen,
            grid=(D // strip,),
            out_shape=widened,
            in_specs=[pl.BlockSpec((nq + 2 * nk, strip), lambda i: (0, i))],
            out_specs=[pl.BlockSpec((n, strip), lambda i: (0, i)) for n in (nq, nk, nk)],
            name="widen",
        )(gw)

    return body


def solution(mesh):
    Z, X, Y, C = 8, 4, mesh.shape["dp"] // 2, 2
    finer = Mesh(mesh.devices.reshape(Z, X, Y, C), ("z", "x", "y", "c"))
    sp, dp = ("z", "x"), ("y", "c")
    return jax.shard_map(
        make_body(Z, X, Y, C),
        mesh=finer,
        in_specs=(P(sp, None), P(dp, None), P(dp, None), P(dp, None), P(), P(), P(sp, dp)),
        out_specs=(P(sp, dp), P(dp, None), P(dp, None), P(dp, None)),
        check_vma=False,
    )
```

```python
import functools

import jax
import jax.numpy as jnp
import numpy as np
from jax import lax
from jax.experimental import pallas as pl
from jax.experimental.pallas import tpu as pltpu
from jax.sharding import Mesh
from jax.sharding import PartitionSpec as P

HEAD_WIDTH = 64
GRID_W = 64
GROUP = 2
CHUNKS = 4
STRIPS = 4
LANES = 128
MESH = pl.DeviceIdType.MESH
F32 = jnp.float32
BF16 = jnp.bfloat16

norm_eps = 1e-06
axial_base = 10000.0

NT = (((1,), (1,)), ((), ()))
NN = (((1,), (0,)), ((), ()))
TN = (((0,), (0,)), ((), ()))


def dot(a, b, dims):
    return lax.dot_general(a, b, dims, preferred_element_type=F32)


def mark(name):
    pass


def rotation_constants(grid_rows):
    quarter = HEAD_WIDTH // 4
    freqs = axial_base ** (-np.arange(quarter, dtype=np.float64) / quarter)
    by_row = np.arange(grid_rows, dtype=np.float64)[:, None] * freqs
    by_col = np.arange(GRID_W, dtype=np.float64)[:, None] * freqs

    def wide(first, second):
        head = np.concatenate([first, first, second, second], axis=1)
        return np.concatenate([head, head], axis=1)

    none_r, none_c = np.zeros_like(by_row), np.zeros_like(by_col)
    rows = np.stack([wide(np.cos(by_row), none_r), wide(np.sin(by_row), none_r)])
    cols = np.stack([wide(none_c, np.cos(by_col)), wide(none_c, np.sin(by_col))])
    return rows.astype(np.float32), cols.astype(np.float32)


def farthest_first(n):
    return sorted(range(1, n), key=lambda d: -min(d, n - d))


def nearest_first(n):
    return sorted(range(1, n), key=lambda d: min(d, n - d))


def kernel(
    sizes, x_ref, wq_ref, wk_ref, wv_ref, qg_hbm, kg_hbm, do_ref, rows_hbm, cols_hbm,
    din_ref, gw_ref,
    qg_ref, kg_ref, rows_ref, cols_ref, w_all, x_buf, kv_buf, q_buf, do_buf, w_buf, e_buf, dp_buf, stat, cfac, delta, st_buf,
    dqt, dkv_send, dkv_buf, dq_send, dq_buf, g_buf, xin, hp_send, hp_buf, gw_part, gwr_buf,
    load_sem, kv_ss, kv_rs, q_ss, q_rs, do_ss, do_rs, st_ss, st_rs, xin_ss, xin_rs, dkv_ss, dkv_rs,
    dq_ss, dq_rs, g_ss, g_rs, hp_ss, hp_rs, gwr_ss, gwr_rs, agz_ss, agz_rs, agx_ss, agx_rs,
):
    Z, X, Y, C, T, D = sizes
    tiles = GROUP * T // LANES
    DX = D // X
    DC = D // (Y * C)
    PZ = LANES // Z
    z, x, y, c = (lax.axis_index(a) for a in ("z", "x", "y", "c"))

    def on_z(d):
        return {"z": lax.rem(z + d, Z)}

    def on_x(d):
        return {"x": lax.rem(x + d, X)}

    def on_dp(dy, dc):
        return {"y": lax.rem(y + dy, Y), "c": lax.rem(c + dc, C)}

    def remote(src, dst, ss, rs, dev):
        return pltpu.make_async_remote_copy(
            src_ref=src, dst_ref=dst, send_sem=ss, recv_sem=rs, device_id=dev, device_id_type=MESH
        )

    dp_pairs = [(dy, dc) for dy in [0] + nearest_first(Y) for dc in range(C) if (dy, dc) != (0, 0)]

    nq, nk = wq_ref.shape[0], wk_ref.shape[0]
    chunk = D // CHUNKS
    sems = iter(range(load_sem.shape[0]))

    def load(src, dst):
        copy = pltpu.make_async_copy(src, dst, load_sem.at[next(sems)])
        copy.start()
        return copy

    mark("a_issue_loads")
    chunk_loads = []
    for i in range(CHUNKS):
        span = pl.ds(i * chunk, chunk)
        chunk_loads.append(
            [
                load(x_ref.at[:, span], x_buf.at[:, span]),
                load(wq_ref.at[:, span], w_all.at[pl.ds(0, nq), span]),
                load(wk_ref.at[:, span], w_all.at[pl.ds(nq, nk), span]),
                load(wv_ref.at[:, span], w_all.at[pl.ds(nq + nk, nk), span]),
            ]
        )
    small_loads = [
        load(rows_hbm, rows_ref),
        load(cols_hbm, cols_ref),
        load(qg_hbm, qg_ref),
        load(kg_hbm, kg_ref),
        load(do_ref, do_buf.at[0]),
    ]
    barrier = pltpu.get_barrier_semaphore()
    for d in range(1, Z):
        pl.semaphore_signal(barrier, inc=1, device_id=on_z(d), device_id_type=MESH)
    for d in range(1, X):
        pl.semaphore_signal(barrier, inc=1, device_id=on_x(d), device_id_type=MESH)
    for dy, dc in dp_pairs:
        pl.semaphore_signal(barrier, inc=1, device_id=on_dp(dy, dc), device_id_type=MESH)

    lane = lax.broadcasted_iota(jnp.int32, (T, LANES), 1)
    low = lax.rem(lane, 32) < 16
    head0 = lane < HEAD_WIDTH
    n_rows = T // GRID_W
    first_row = (z * X + x) * n_rows

    def table(k):
        return jnp.concatenate(
            [rows_ref[k, pl.ds(first_row + j, 1), :] + cols_ref[k] for j in range(n_rows)], axis=0
        )

    def turned(v):
        return jnp.where(low, pltpu.roll(v, LANES - 16, 1), pltpu.roll(v, 16, 1))

    def rotate(v):
        return v * cos + turned(v) * sin

    def rotate_back(v):
        return v * cos - turned(v) * sin

    def head_mean(v):
        first = jnp.sum(jnp.where(head0, v, 0.0), axis=1, keepdims=True)
        second = jnp.sum(jnp.where(head0, 0.0, v), axis=1, keepdims=True)
        return jnp.where(head0, first, second) * (1.0 / HEAD_WIDTH)

    mark("b_proj")
    raw = jnp.zeros((T, 2 * LANES), F32)
    for i, group in enumerate(chunk_loads):
        for copy in group:
            copy.wait()
        raw = raw + dot(x_buf[:, i * chunk : (i + 1) * chunk], w_all[:, i * chunk : (i + 1) * chunk], NT)
    raw = raw.astype(BF16).astype(F32)
    for copy in small_loads:
        copy.wait()
    qg = jnp.concatenate([qg_ref[...], qg_ref[...]], axis=1)
    kg = jnp.concatenate([kg_ref[...], kg_ref[...]], axis=1)
    cos = table(0)
    sin = table(1)
    sin = jnp.where(low, -sin, sin)

    kv_raw = raw[:, LANES:]
    k_inv = lax.rsqrt(head_mean(kv_raw * kv_raw) + norm_eps)
    k_hat = kv_raw * k_inv
    kv_buf[0] = jnp.where(head0, rotate(k_hat * kg), kv_raw).astype(BF16)

    mark("c_barrier")
    pl.semaphore_wait(barrier, (Z - 1) + (X - 1) + len(dp_pairs))

    mark("d_issue")
    kv_copies, q_copies, do_copies, xin_copies = {}, {}, {}, {}
    for d in nearest_first(Z):
        kv_copies[d] = remote(kv_buf.at[0], kv_buf.at[d], kv_ss.at[d], kv_rs.at[d], on_z(d))
        kv_copies[d].start()
    q_raw = raw[:, :LANES]
    q_inv = lax.rsqrt(head_mean(q_raw * q_raw) + norm_eps)
    q_hat = q_raw * q_inv
    q_buf[0] = rotate(q_hat * qg).astype(BF16)
    for d in nearest_first(X):
        q_copies[d] = remote(q_buf.at[0], q_buf.at[d], q_ss.at[d], q_rs.at[d], on_x(d))
        q_copies[d].start()
        do_copies[d] = remote(do_buf.at[0], do_buf.at[d], do_ss.at[d], do_rs.at[d], on_x(d))
        do_copies[d].start()

    def send_columns(d):
        cols = pl.multiple_of(lax.rem(x + d, X) * DX, LANES)
        xin_copies[d] = remote(
            x_buf.at[:, pl.ds(cols, DX)], xin.at[d], xin_ss.at[d], xin_rs.at[d], on_x(d)
        )
        xin_copies[d].start()

    near = [d for d in nearest_first(X) if min(d, X - d) == 1]
    for d in near:
        send_columns(d)

    def src_x(d):
        return lax.rem(x + X - d, X)

    def take_queries(d):
        if d:
            mark(f"e_qwait{d}")
            q_copies[d].wait()
            do_copies[d].wait()
        mark(f"f_build{d}")
        q_rows = q_buf[d].astype(F32) * (HEAD_WIDTH**-0.5)
        do_rows = do_buf[d].astype(F32)
        qa = jnp.concatenate(
            [jnp.where(head0, q_rows, 0.0), jnp.where(head0, pltpu.roll(q_rows, HEAD_WIDTH, 1), 0.0)], axis=0
        ).astype(BF16)
        doa = jnp.concatenate(
            [jnp.where(head0, 0.0, pltpu.roll(do_rows, HEAD_WIDTH, 1)), jnp.where(head0, 0.0, do_rows)], axis=0
        ).astype(BF16)
        for t in range(tiles):
            w_buf[d, t, 0:LANES] = qa[t * LANES : (t + 1) * LANES]
            w_buf[d, t, LANES:] = doa[t * LANES : (t + 1) * LANES]

    def take_keys(d):
        if d:
            mark(f"g_kvwait{d}")
            kv_copies[d].wait()

    def forward(d, q):
        kv = kv_buf[d]
        for t in range(tiles):
            both = dot(kv, w_buf[q, t], NT)
            s = both[:, :LANES]
            dp = both[:, LANES:]
            m = jnp.max(s, axis=0, keepdims=True)
            e = jnp.exp(s - m)
            stat[d, q, t, 0] = m
            stat[d, q, t, 1] = jnp.sum(e, axis=0, keepdims=True)
            stat[d, q, t, 2] = jnp.sum(e * dp, axis=0, keepdims=True)
            e_buf[d, q, t] = e
            dp_buf[d, q, t] = dp

    arrivals = []
    zs, xs = [0] + nearest_first(Z), [0] + nearest_first(X)
    order = [("k", 0, 0.0), ("q", 0, 0.0)]
    order += [("k", d, 1.0 + 2.0 * min(d, Z - d) - (d < Z - d) * 0.1) for d in zs[1:]]
    order += [("q", d, 3.5 + 3.0 * (min(d, X - d) - 1) - (d < X - d) * 0.1) for d in xs[1:]]
    keys_in, queries_in = [], []
    for kind, d, _ in sorted(order, key=lambda item: item[2]):
        if kind == "k":
            take_keys(d)
            keys_in.append(d)
            blocks = [(d, q) for q in queries_in]
        else:
            take_queries(d)
            queries_in.append(d)
            blocks = [(k, d) for k in keys_in]
        if blocks:
            mark(f"h_fwd_{kind}{d}")
        for k, q in blocks:
            forward(k, q)

    def merged(parts):
        top = parts[0][0]
        for m, _, _ in parts[1:]:
            top = jnp.maximum(top, m)
        total, weighted = jnp.zeros_like(top), jnp.zeros_like(top)
        for m, l, w in parts:
            f = jnp.exp(m - top)
            total = total + l * f
            weighted = weighted + w * f
        return top, total, weighted

    mark("i_stat")
    for q in range(X):
        parts = [[stat[d, q, :, i] for i in range(3)] for d in range(Z)]
        for i, value in enumerate(merged(parts)):
            st_buf[0, src_x(q), i] = value
    st_copies = {}
    for d in nearest_first(X):
        st_copies[d] = remote(st_buf.at[0], st_buf.at[d], st_ss.at[d], st_rs.at[d], on_x(d))
        st_copies[d].start()
    for d in nearest_first(X):
        if d not in near:
            send_columns(d)
    mark("j_stwait")
    for d in range(1, X):
        st_copies[d].wait()
    mark("k_comb")
    for q in range(X):
        at = src_x(q)
        top, total, weighted = merged([[st_buf[d, at, i] for i in range(3)] for d in range(X)])
        log_total = top + jnp.log(total)
        delta[q] = weighted / total
        for d in range(Z):
            cfac[d, q] = jnp.exp(stat[d, q, :, 0] - log_total)

    dqt[...] = jnp.zeros_like(dqt)
    dkv_copies = {}
    dkv_own = None
    for d in farthest_first(Z) + [0]:
        mark(f"l_bwd{d}")
        k_t = kv_buf[d].astype(F32).T[:HEAD_WIDTH].astype(BF16)

        acc = jnp.zeros((T, LANES), F32)
        for q in range(X):
            scores_grad = []
            for t in range(tiles):
                p = e_buf[d, q, t] * cfac[d, q, t]
                ds = (p * (dp_buf[d, q, t] - delta[q, t])).astype(BF16)
                scores_grad.append(ds)
                acc = acc + dot(jnp.concatenate([ds, p.astype(BF16)], axis=1), w_buf[q, t], NN)
            dqt[q] += dot(k_t, jnp.concatenate(scores_grad, axis=1), NN)
        if d:
            dkv_send[d] = acc.astype(BF16)
            dkv_copies[d] = remote(
                dkv_send.at[d], dkv_buf.at[d], dkv_ss.at[d], dkv_rs.at[d], on_z(Z - d)
            )
            dkv_copies[d].start()
        else:
            dkv_own = acc

    mark("m_dq")
    dq_copies = {}

    def dq_of(q):
        rows = dqt[q].T
        return jnp.concatenate([rows[:T], rows[T:]], axis=1)

    for d in nearest_first(X):
        dq_send[d] = dq_of(d).astype(BF16)
        dq_copies[d] = remote(
            dq_send.at[d], dq_buf.at[d], dq_ss.at[d], dq_rs.at[d], on_x(X - d)
        )
        dq_copies[d].start()
    dq_own = dq_of(0)

    def norm_back(grads, normed, inv, gain):
        u = rotate_back(grads) * gain
        return inv * (u - normed * head_mean(u * normed))

    g_copies = {}

    def send_grads(part, value):
        g_buf[0, part] = value
        for d in nearest_first(X):
            g_copies[d, part] = remote(
                g_buf.at[0, part], g_buf.at[d, part], g_ss.at[d, part], g_rs.at[d, part], on_x(d)
            )
            g_copies[d, part].start()

    mark("n_dqwait")
    for d in range(1, X):
        dq_copies[d].wait()
        dq_own = dq_own + dq_buf[d].astype(F32)
    mark("n_normq")
    grad_q = norm_back(dq_own * (HEAD_WIDTH**-0.5), q_hat, q_inv, qg).astype(BF16)
    send_grads(0, grad_q)
    mark("o_dkvwait")
    for d in range(1, Z):
        dkv_copies[d].wait()
        dkv_own = dkv_own + dkv_buf[d].astype(F32)
    mark("p_normk")
    grad_k = norm_back(jnp.where(head0, dkv_own, 0.0), k_hat, k_inv, kg)
    grad_kv = jnp.where(head0, grad_k, dkv_own).astype(BF16)
    send_grads(1, grad_kv)

    mark("q_hp")
    g = jnp.concatenate([grad_q, grad_kv], axis=1)
    for j in range(0, Y * C, 2):
        two = dot(g, w_all[:, j * DC : (j + 2) * DC], NN).astype(BF16)
        hp_send[j] = two[:, :DC]
        hp_send[j + 1] = two[:, DC:]
    hp_copies = {}
    for dy, dc in reversed(dp_pairs):
        slot = dy * C + dc
        column = lax.rem(y + dy, Y) * C + lax.rem(c + dc, C)
        hp_copies[slot] = remote(
            hp_send.at[column], hp_buf.at[slot], hp_ss.at[slot], hp_rs.at[slot], on_dp(dy, dc)
        )
        hp_copies[slot].start()

    cols = pl.multiple_of(x * DX, LANES)
    gwr_copies, agz_copies, agx_copies = {}, {}, {}

    def multiply(part):
        gw = dot(g_buf[0, part], x_buf[:, pl.ds(cols, DX)], TN)
        for d in nearest_first(X):
            g_copies[d, part].wait()
            if not part:
                xin_copies[d].wait()
            gw = gw + dot(g_buf[d, part], xin[d], TN)
        gw_part[part] = gw.astype(BF16)
        for d in farthest_first(Z):
            rows = pl.multiple_of(lax.rem(z + d, Z) * PZ, PZ)
            gwr_copies[d, part] = remote(
                gw_part.at[part, pl.ds(rows, PZ)], gwr_buf.at[part, d],
                gwr_ss.at[d, part], gwr_rs.at[d, part], on_z(d),
            )
            gwr_copies[d, part].start()

    def region(part, dz):
        rows = pl.multiple_of(part * LANES + lax.rem(z + Z - dz, Z) * PZ, PZ)
        return gw_ref.at[pl.ds(rows, PZ), pl.ds(cols, DX)]

    def pass_on(part, dz):
        block = region(part, dz)
        for d in nearest_first(X):
            copy = remote(block, block, agx_ss.at[d, dz, part], agx_rs.at[d, dz, part], on_x(d))
            copy.start()
            agx_copies[part, dz, d] = copy

    def add_up(part):
        my_rows = pl.multiple_of(z * PZ, PZ)
        piece = gw_part[part, pl.ds(my_rows, PZ), :].astype(F32)
        for d in farthest_first(Z):
            gwr_copies[d, part].wait()
            piece = piece + gwr_buf[part, d].astype(F32)
        gw_ref[pl.ds(pl.multiple_of(part * LANES + my_rows, PZ), PZ), pl.ds(cols, DX)] = piece.astype(BF16)
        own = region(part, 0)
        for d in farthest_first(Z):
            agz_copies[part, d] = remote(own, own, agz_ss.at[d, part], agz_rs.at[d, part], on_z(d))
            agz_copies[part, d].start()
        pass_on(part, 0)

    for part in range(2):
        mark(f"r_gw{part}")
        multiply(part)
    for part in range(2):
        mark(f"s_gwrwait{part}")
        add_up(part)
    for part in range(2):
        mark(f"t_agz{part}")
        for dz in nearest_first(Z):
            agz_copies[part, dz].wait_recv()
            pass_on(part, dz)

    mark("u_hpwait")
    din = hp_send[y * C + c].astype(F32)
    for slot, copy in hp_copies.items():
        copy.wait()
        din = din + hp_buf[slot].astype(F32)
    din_ref[...] = din.astype(BF16)
    mark("v_agxwait")
    for copy in agx_copies.values():
        copy.wait()
    for copy in agz_copies.values():
        copy.wait_send()
    mark(None)


def widen(gw_ref, din_ref, *refs):
    *grad_refs, din_out, wide, sems = refs
    last = pltpu.make_async_copy(din_ref, din_out, sems.at[STRIPS, 0])
    last.start()
    copies = [last]
    strip = gw_ref.shape[1] // STRIPS
    for i in range(STRIPS):
        span = pl.ds(i * strip, strip)
        wide[:, span] = gw_ref[:, span].astype(F32)
        first = 0
        for k, ref in enumerate(grad_refs):
            rows = ref.shape[0]
            copy = pltpu.make_async_copy(
                wide.at[pl.ds(first, rows), span], ref.at[:, span], sems.at[i, k]
            )
            copy.start()
            copies.append(copy)
            first += rows
    for copy in copies:
        copy.wait()


def make_body(Z, X, Y, C):
    def body(inputs, w_query, w_key, w_value, query_gain, key_gain, grad_out):
        T, D = inputs.shape
        nq, nk = w_query.shape[0], w_key.shape[0]
        rows, cols = rotation_constants(Z * X * T // GRID_W)
        DX, DC, PZ = D // X, D // (Y * C), LANES // Z
        sizes = (Z, X, Y, C, T, D)
        tiles = GROUP * T // LANES
        dma = pltpu.SemaphoreType.DMA
        pair = lambda *n: [dma(n), dma(n)]
        vmem = pl.BlockSpec(memory_space=pltpu.VMEM)
        hbm = pl.BlockSpec(memory_space=pltpu.HBM)
        din, gw = pl.pallas_call(
            functools.partial(kernel, sizes),
            out_shape=(
                jax.ShapeDtypeStruct((T, DC), BF16),
                jax.ShapeDtypeStruct((nq + 2 * nk, D), BF16),
            ),
            in_specs=[hbm] * 9,
            out_specs=(vmem, vmem),
            scratch_shapes=[
                pltpu.VMEM((1, HEAD_WIDTH), F32),
                pltpu.VMEM((1, HEAD_WIDTH), F32),
                pltpu.VMEM(rows.shape, F32),
                pltpu.VMEM(cols.shape, F32),
                pltpu.VMEM((nq + 2 * nk, D), BF16),
                pltpu.VMEM((T, D), BF16),
                pltpu.VMEM((Z, T, LANES), BF16),
                pltpu.VMEM((X, T, LANES), BF16),
                pltpu.VMEM((X, T, LANES), BF16),
                pltpu.VMEM((X, tiles, 2 * LANES, LANES), BF16),
                pltpu.VMEM((Z, X, tiles, T, LANES), F32),
                pltpu.VMEM((Z, X, tiles, T, LANES), F32),
                pltpu.VMEM((Z, X, tiles, 3, 1, LANES), F32),
                pltpu.VMEM((Z, X, tiles, 1, LANES), F32),
                pltpu.VMEM((X, tiles, 1, LANES), F32),
                pltpu.VMEM((X, X, 3, tiles, 1, LANES), F32),
                pltpu.VMEM((X, HEAD_WIDTH, GROUP * T), F32),
                pltpu.VMEM((Z, T, LANES), BF16),
                pltpu.VMEM((Z, T, LANES), BF16),
                pltpu.VMEM((X, T, LANES), BF16),
                pltpu.VMEM((X, T, LANES), BF16),
                pltpu.VMEM((X, 2, T, LANES), BF16),
                pltpu.VMEM((X, T, DX), BF16),
                pltpu.VMEM((Y * C, T, DC), BF16),
                pltpu.VMEM((Y * C, T, DC), BF16),
                pltpu.VMEM((2, LANES, DX), BF16),
                pltpu.VMEM((2, Z, PZ, DX), BF16),
                dma((4 * CHUNKS + 5,)),
                *pair(Z), *pair(X), *pair(X), *pair(X), *pair(X), *pair(Z),
                *pair(X), *pair(X, 2), *pair(Y * C), *pair(Z, 2), *pair(Z, 2), *pair(X, Z, 2),
            ],
            compiler_params=pltpu.CompilerParams(
                collective_id=0, has_side_effects=True, vmem_limit_bytes=40 * 1024 * 1024
            ),
            name="attention_backward",
        )(
            *[
                pltpu.with_memory_space_constraint(a, pltpu.HBM)
                for a in (
                    inputs, w_query, w_key, w_value, query_gain.reshape(1, -1),
                    key_gain.reshape(1, -1), grad_out, jnp.asarray(rows), jnp.asarray(cols),
                )
            ]
        )
        rest = [jax.ShapeDtypeStruct((n, D), F32) for n in (nq, nk, nk)]
        *grads, din = pl.pallas_call(
            widen,
            out_shape=[*rest, jax.ShapeDtypeStruct((T, DC), BF16)],
            in_specs=[vmem, vmem],
            out_specs=[hbm] * 4,
            scratch_shapes=[pltpu.VMEM((nq + 2 * nk, D), F32), dma((STRIPS + 1, 3))],
            compiler_params=pltpu.CompilerParams(vmem_limit_bytes=16 * 1024 * 1024),
            name="widen",
        )(gw, din)
        return din, *grads

    return body


def solution(mesh):
    Z, X, Y, C = 8, 4, mesh.shape["dp"] // 2, 2
    finer = Mesh(mesh.devices.reshape(Z, X, Y, C), ("z", "x", "y", "c"))
    sp, dp = ("z", "x"), ("y", "c")
    return jax.shard_map(
        make_body(Z, X, Y, C),
        mesh=finer,
        in_specs=(P(sp, None), P(dp, None), P(dp, None), P(dp, None), P(), P(), P(sp, dp)),
        out_specs=(P(sp, dp), P(dp, None), P(dp, None), P(dp, None)),
        check_vma=False,
    )
```

```python
import functools

import jax
import jax.numpy as jnp
import numpy as np
from jax import lax
from jax.experimental import pallas as pl
from jax.experimental.pallas import tpu as pltpu
from jax.sharding import Mesh
from jax.sharding import PartitionSpec as P

HEAD_WIDTH = 64
GRID_W = 64
GROUP = 2
CHUNKS = 4
STRIPS = 4
LANES = 128
MESH = pl.DeviceIdType.MESH
F32 = jnp.float32
BF16 = jnp.bfloat16

norm_eps = 1e-06
axial_base = 10000.0

NT = (((1,), (1,)), ((), ()))
NN = (((1,), (0,)), ((), ()))
TN = (((0,), (0,)), ((), ()))


def dot(a, b, dims):
    return lax.dot_general(a, b, dims, preferred_element_type=F32)


def mark(name):
    pass


def rotation_constants(grid_rows):
    quarter = HEAD_WIDTH // 4
    freqs = axial_base ** (-np.arange(quarter, dtype=np.float64) / quarter)
    by_row = np.arange(grid_rows, dtype=np.float64)[:, None] * freqs
    by_col = np.arange(GRID_W, dtype=np.float64)[:, None] * freqs

    def wide(first, second):
        head = np.concatenate([first, first, second, second], axis=1)
        return np.concatenate([head, head], axis=1)

    none_r, none_c = np.zeros_like(by_row), np.zeros_like(by_col)
    rows = np.stack([wide(np.cos(by_row), none_r), wide(np.sin(by_row), none_r)])
    cols = np.stack([wide(none_c, np.cos(by_col)), wide(none_c, np.sin(by_col))])
    return rows.astype(np.float32), cols.astype(np.float32)


def farthest_first(n):
    return sorted(range(1, n), key=lambda d: -min(d, n - d))


def nearest_first(n):
    return sorted(range(1, n), key=lambda d: min(d, n - d))


def kernel(
    sizes, x_ref, wq_ref, wk_ref, wv_ref, qg_hbm, kg_hbm, do_ref, rows_hbm, cols_hbm,
    din_ref, gw_ref,
    qg_ref, kg_ref, rows_ref, cols_ref, w_all, x_buf, kv_buf, q_buf, do_buf, w_buf, e_buf, dp_buf, stat, cfac, delta, st_buf,
    dqt, dkv_send, dkv_buf, dq_send, dq_buf, g_buf, xin, hp_send, hp_pair, hp_sum, hp_buf, gw_part, gwr_buf,
    load_sem, kv_ss, kv_rs, q_ss, q_rs, do_ss, do_rs, st_ss, st_rs, xin_ss, xin_rs, dkv_ss, dkv_rs,
    dq_ss, dq_rs, g_ss, g_rs, hp_ss, hp_rs, gwr_ss, gwr_rs, agz_ss, agz_rs, agx_ss, agx_rs,
):
    Z, X, Y, C, T, D = sizes
    tiles = GROUP * T // LANES
    DX = D // X
    DC = D // (Y * C)
    PZ = LANES // Z
    z, x, y, c = (lax.axis_index(a) for a in ("z", "x", "y", "c"))

    def on_z(d):
        return {"z": lax.rem(z + d, Z)}

    def on_x(d):
        return {"x": lax.rem(x + d, X)}

    def on_y(d):
        return {"y": lax.rem(y + d, Y)}

    def remote(src, dst, ss, rs, dev):
        return pltpu.make_async_remote_copy(
            src_ref=src, dst_ref=dst, send_sem=ss, recv_sem=rs, device_id=dev, device_id_type=MESH
        )

    nq, nk = wq_ref.shape[0], wk_ref.shape[0]
    chunk = D // CHUNKS
    sems = iter(range(load_sem.shape[0]))

    def load(src, dst):
        copy = pltpu.make_async_copy(src, dst, load_sem.at[next(sems)])
        copy.start()
        return copy

    mark("a_issue_loads")
    chunk_loads = []
    for i in range(CHUNKS):
        span = pl.ds(i * chunk, chunk)
        chunk_loads.append(
            [
                load(x_ref.at[:, span], x_buf.at[:, span]),
                load(wq_ref.at[:, span], w_all.at[pl.ds(0, nq), span]),
                load(wk_ref.at[:, span], w_all.at[pl.ds(nq, nk), span]),
                load(wv_ref.at[:, span], w_all.at[pl.ds(nq + nk, nk), span]),
            ]
        )
    small_loads = [
        load(rows_hbm, rows_ref),
        load(cols_hbm, cols_ref),
        load(qg_hbm, qg_ref),
        load(kg_hbm, kg_ref),
        load(do_ref, do_buf.at[0]),
    ]
    barrier = pltpu.get_barrier_semaphore()
    for d in range(1, Z):
        pl.semaphore_signal(barrier, inc=1, device_id=on_z(d), device_id_type=MESH)
    for d in range(1, X):
        pl.semaphore_signal(barrier, inc=1, device_id=on_x(d), device_id_type=MESH)
    for d in range(1, Y):
        pl.semaphore_signal(barrier, inc=1, device_id=on_y(d), device_id_type=MESH)
    pl.semaphore_signal(barrier, inc=1, device_id={"c": 1 - c}, device_id_type=MESH)

    lane = lax.broadcasted_iota(jnp.int32, (T, LANES), 1)
    low = lax.rem(lane, 32) < 16
    head0 = lane < HEAD_WIDTH
    n_rows = T // GRID_W
    first_row = (z * X + x) * n_rows

    def table(k):
        return jnp.concatenate(
            [rows_ref[k, pl.ds(first_row + j, 1), :] + cols_ref[k] for j in range(n_rows)], axis=0
        )

    def turned(v):
        return jnp.where(low, pltpu.roll(v, LANES - 16, 1), pltpu.roll(v, 16, 1))

    def rotate(v):
        return v * cos + turned(v) * sin

    def rotate_back(v):
        return v * cos - turned(v) * sin

    def head_mean(v):
        first = jnp.sum(jnp.where(head0, v, 0.0), axis=1, keepdims=True)
        second = jnp.sum(jnp.where(head0, 0.0, v), axis=1, keepdims=True)
        return jnp.where(head0, first, second) * (1.0 / HEAD_WIDTH)

    mark("b_proj")
    raw = jnp.zeros((T, 2 * LANES), F32)
    for i, group in enumerate(chunk_loads):
        for copy in group:
            copy.wait()
        raw = raw + dot(x_buf[:, i * chunk : (i + 1) * chunk], w_all[:, i * chunk : (i + 1) * chunk], NT)
    raw = raw.astype(BF16).astype(F32)
    for copy in small_loads:
        copy.wait()
    qg = jnp.concatenate([qg_ref[...], qg_ref[...]], axis=1)
    kg = jnp.concatenate([kg_ref[...], kg_ref[...]], axis=1)
    cos = table(0)
    sin = table(1)
    sin = jnp.where(low, -sin, sin)

    kv_raw = raw[:, LANES:]
    k_inv = lax.rsqrt(head_mean(kv_raw * kv_raw) + norm_eps)
    k_hat = kv_raw * k_inv
    kv_buf[0] = jnp.where(head0, rotate(k_hat * kg), kv_raw).astype(BF16)

    mark("c_barrier")
    pl.semaphore_wait(barrier, (Z - 1) + (X - 1) + (Y - 1) + 1)

    mark("d_issue")
    kv_copies, q_copies, do_copies, xin_copies = {}, {}, {}, {}
    for d in nearest_first(Z):
        kv_copies[d] = remote(kv_buf.at[0], kv_buf.at[d], kv_ss.at[d], kv_rs.at[d], on_z(d))
        kv_copies[d].start()
    q_raw = raw[:, :LANES]
    q_inv = lax.rsqrt(head_mean(q_raw * q_raw) + norm_eps)
    q_hat = q_raw * q_inv
    q_buf[0] = rotate(q_hat * qg).astype(BF16)
    for d in nearest_first(X):
        q_copies[d] = remote(q_buf.at[0], q_buf.at[d], q_ss.at[d], q_rs.at[d], on_x(d))
        q_copies[d].start()
        do_copies[d] = remote(do_buf.at[0], do_buf.at[d], do_ss.at[d], do_rs.at[d], on_x(d))
        do_copies[d].start()

    def send_columns(d):
        cols = pl.multiple_of(lax.rem(x + d, X) * DX, LANES)
        xin_copies[d] = remote(
            x_buf.at[:, pl.ds(cols, DX)], xin.at[d], xin_ss.at[d], xin_rs.at[d], on_x(d)
        )
        xin_copies[d].start()

    near = [d for d in nearest_first(X) if min(d, X - d) == 1]
    for d in near:
        send_columns(d)

    def src_x(d):
        return lax.rem(x + X - d, X)

    def take_queries(d):
        if d:
            mark(f"e_qwait{d}")
            q_copies[d].wait()
            do_copies[d].wait()
        mark(f"f_build{d}")
        q_rows = q_buf[d].astype(F32) * (HEAD_WIDTH**-0.5)
        do_rows = do_buf[d].astype(F32)
        qa = jnp.concatenate(
            [jnp.where(head0, q_rows, 0.0), jnp.where(head0, pltpu.roll(q_rows, HEAD_WIDTH, 1), 0.0)], axis=0
        ).astype(BF16)
        doa = jnp.concatenate(
            [jnp.where(head0, 0.0, pltpu.roll(do_rows, HEAD_WIDTH, 1)), jnp.where(head0, 0.0, do_rows)], axis=0
        ).astype(BF16)
        for t in range(tiles):
            w_buf[d, t, 0:LANES] = qa[t * LANES : (t + 1) * LANES]
            w_buf[d, t, LANES:] = doa[t * LANES : (t + 1) * LANES]

    def take_keys(d):
        if d:
            mark(f"g_kvwait{d}")
            kv_copies[d].wait()

    def forward(d, q):
        kv = kv_buf[d]
        for t in range(tiles):
            both = dot(kv, w_buf[q, t], NT)
            s = both[:, :LANES]
            dp = both[:, LANES:]
            m = jnp.max(s, axis=0, keepdims=True)
            e = jnp.exp(s - m)
            stat[d, q, t, 0] = m
            stat[d, q, t, 1] = jnp.sum(e, axis=0, keepdims=True)
            stat[d, q, t, 2] = jnp.sum(e * dp, axis=0, keepdims=True)
            e_buf[d, q, t] = e
            dp_buf[d, q, t] = dp

    arrivals = []
    zs, xs = [0] + nearest_first(Z), [0] + nearest_first(X)
    order = [("k", 0, 0.0), ("q", 0, 0.0)]
    order += [("k", d, 1.0 + 2.0 * min(d, Z - d) - (d < Z - d) * 0.1) for d in zs[1:]]
    order += [("q", d, 3.5 + 3.0 * (min(d, X - d) - 1) - (d < X - d) * 0.1) for d in xs[1:]]
    keys_in, queries_in = [], []
    for kind, d, _ in sorted(order, key=lambda item: item[2]):
        if kind == "k":
            take_keys(d)
            keys_in.append(d)
            blocks = [(d, q) for q in queries_in]
        else:
            take_queries(d)
            queries_in.append(d)
            blocks = [(k, d) for k in keys_in]
        if blocks:
            mark(f"h_fwd_{kind}{d}")
        for k, q in blocks:
            forward(k, q)

    def merged(parts):
        top = parts[0][0]
        for m, _, _ in parts[1:]:
            top = jnp.maximum(top, m)
        total, weighted = jnp.zeros_like(top), jnp.zeros_like(top)
        for m, l, w in parts:
            f = jnp.exp(m - top)
            total = total + l * f
            weighted = weighted + w * f
        return top, total, weighted

    mark("i_stat")
    for q in range(X):
        parts = [[stat[d, q, :, i] for i in range(3)] for d in range(Z)]
        for i, value in enumerate(merged(parts)):
            st_buf[0, src_x(q), i] = value
    st_copies = {}
    for d in farthest_first(X):
        st_copies[d] = remote(st_buf.at[0], st_buf.at[d], st_ss.at[d], st_rs.at[d], on_x(d))
        st_copies[d].start()
    for d in nearest_first(X):
        if d not in near:
            send_columns(d)
    mark("j_stwait")
    for d in range(1, X):
        st_copies[d].wait()
    mark("k_comb")
    for q in range(X):
        at = src_x(q)
        top, total, weighted = merged([[st_buf[d, at, i] for i in range(3)] for d in range(X)])
        log_total = top + jnp.log(total)
        delta[q] = weighted / total
        for d in range(Z):
            cfac[d, q] = jnp.exp(stat[d, q, :, 0] - log_total)

    dqt[...] = jnp.zeros_like(dqt)
    dkv_copies = {}
    dkv_own = None
    for d in farthest_first(Z) + [0]:
        mark(f"l_bwd{d}")
        k_t = kv_buf[d].astype(F32).T[:HEAD_WIDTH].astype(BF16)

        acc = jnp.zeros((T, LANES), F32)
        for q in range(X):
            scores_grad = []
            for t in range(tiles):
                p = e_buf[d, q, t] * cfac[d, q, t]
                ds = (p * (dp_buf[d, q, t] - delta[q, t])).astype(BF16)
                scores_grad.append(ds)
                acc = acc + dot(jnp.concatenate([ds, p.astype(BF16)], axis=1), w_buf[q, t], NN)
            dqt[q] += dot(k_t, jnp.concatenate(scores_grad, axis=1), NN)
        if d:
            dkv_send[d] = acc.astype(BF16)
            dkv_copies[d] = remote(
                dkv_send.at[d], dkv_buf.at[d], dkv_ss.at[d], dkv_rs.at[d], on_z(Z - d)
            )
            dkv_copies[d].start()
        else:
            dkv_own = acc

    mark("m_dq")
    dq_copies = {}

    def dq_of(q):
        rows = dqt[q].T
        return jnp.concatenate([rows[:T], rows[T:]], axis=1)

    for d in farthest_first(X):
        dq_send[d] = dq_of(d).astype(BF16)
        dq_copies[d] = remote(
            dq_send.at[d], dq_buf.at[d], dq_ss.at[d], dq_rs.at[d], on_x(X - d)
        )
        dq_copies[d].start()
    dq_own = dq_of(0)

    def norm_back(grads, normed, inv, gain):
        u = rotate_back(grads) * gain
        return inv * (u - normed * head_mean(u * normed))

    g_copies = {}

    def send_grads(part, value):
        g_buf[0, part] = value
        for d in farthest_first(X):
            g_copies[d, part] = remote(
                g_buf.at[0, part], g_buf.at[d, part], g_ss.at[d, part], g_rs.at[d, part], on_x(d)
            )
            g_copies[d, part].start()

    mark("n_dqwait")
    for d in range(1, X):
        dq_copies[d].wait()
        dq_own = dq_own + dq_buf[d].astype(F32)
    mark("n_normq")
    grad_q = norm_back(dq_own * (HEAD_WIDTH**-0.5), q_hat, q_inv, qg).astype(BF16)
    send_grads(0, grad_q)
    mark("o_dkvwait")
    for d in range(1, Z):
        dkv_copies[d].wait()
        dkv_own = dkv_own + dkv_buf[d].astype(F32)
    mark("p_normk")
    grad_k = norm_back(jnp.where(head0, dkv_own, 0.0), k_hat, k_inv, kg)
    grad_kv = jnp.where(head0, grad_k, dkv_own).astype(BF16)
    send_grads(1, grad_kv)

    mark("q_hp")
    g = jnp.concatenate([grad_q, grad_kv], axis=1)
    for j in range(Y):
        two = dot(g, w_all[:, j * C * DC : (j + 1) * C * DC], NN).astype(BF16)
        for k in range(C):
            hp_send[k, j] = two[:, k * DC : (k + 1) * DC]
    pair_copy = remote(hp_send.at[1 - c], hp_pair, hp_ss.at[0], hp_rs.at[0], {"c": 1 - c})
    pair_copy.start()
    hp_copies = {}

    def send_parts():
        mark("q_pair")
        pair_copy.wait()
        for j in range(Y):
            hp_sum[j] = (hp_send[c, j].astype(F32) + hp_pair[j].astype(F32)).astype(BF16)
        for d in farthest_first(Y):
            hp_copies[d] = remote(
                hp_sum.at[lax.rem(y + d, Y)], hp_buf.at[d], hp_ss.at[d], hp_rs.at[d], on_y(d)
            )
            hp_copies[d].start()

    cols = pl.multiple_of(x * DX, LANES)
    gwr_copies, agz_copies, agx_copies = {}, {}, {}

    def multiply(part):
        gw = dot(g_buf[0, part], x_buf[:, pl.ds(cols, DX)], TN)
        for d in nearest_first(X):
            g_copies[d, part].wait()
            if not part:
                xin_copies[d].wait()
            gw = gw + dot(g_buf[d, part], xin[d], TN)
        gw_part[part] = gw.astype(BF16)
        for d in farthest_first(Z):
            rows = pl.multiple_of(lax.rem(z + d, Z) * PZ, PZ)
            gwr_copies[d, part] = remote(
                gw_part.at[part, pl.ds(rows, PZ)], gwr_buf.at[part, d],
                gwr_ss.at[d, part], gwr_rs.at[d, part], on_z(d),
            )
            gwr_copies[d, part].start()

    def region(part, dz):
        rows = pl.multiple_of(part * LANES + lax.rem(z + Z - dz, Z) * PZ, PZ)
        return gw_ref.at[pl.ds(rows, PZ), pl.ds(cols, DX)]

    def pass_on(part, dz):
        block = region(part, dz)
        for d in farthest_first(X):
            copy = remote(block, block, agx_ss.at[d, dz, part], agx_rs.at[d, dz, part], on_x(d))
            copy.start()
            agx_copies[part, dz, d] = copy

    def add_up(part):
        my_rows = pl.multiple_of(z * PZ, PZ)
        piece = gw_part[part, pl.ds(my_rows, PZ), :].astype(F32)
        for d in farthest_first(Z):
            gwr_copies[d, part].wait()
            piece = piece + gwr_buf[part, d].astype(F32)
        gw_ref[
            pl.ds(pl.multiple_of(part * LANES + my_rows, PZ), PZ),
            pl.ds(cols, DX),
        ] = piece.astype(BF16)
        own = region(part, 0)
        for d in farthest_first(Z):
            agz_copies[part, d] = remote(own, own, agz_ss.at[d, part], agz_rs.at[d, part], on_z(d))
            agz_copies[part, d].start()
        pass_on(part, 0)

    for part in range(2):
        mark(f"r_gw{part}")
        multiply(part)
        if part == 0:
            send_parts()
    for part in range(2):
        mark(f"s_gwrwait{part}")
        add_up(part)
    for part in range(2):
        mark(f"t_agz{part}")
        for dz in nearest_first(Z):
            agz_copies[part, dz].wait_recv()
            pass_on(part, dz)
    mark("u_hpwait")
    din = hp_sum[y].astype(F32)
    for d, copy in hp_copies.items():
        copy.wait()
        din = din + hp_buf[d].astype(F32)
    din_ref[...] = din.astype(BF16)
    mark("v_agxwait")
    for copy in agx_copies.values():
        copy.wait()
    for copy in agz_copies.values():
        copy.wait_send()
    mark(None)


def widen(gw_ref, din_ref, *refs):
    *grad_refs, din_out, wide, sems = refs
    last = pltpu.make_async_copy(din_ref, din_out, sems.at[STRIPS, 0])
    last.start()
    copies = [last]
    strip = gw_ref.shape[1] // STRIPS
    for i in range(STRIPS):
        span = pl.ds(i * strip, strip)
        wide[:, span] = gw_ref[:, span].astype(F32)
        first = 0
        for k, ref in enumerate(grad_refs):
            rows = ref.shape[0]
            copy = pltpu.make_async_copy(
                wide.at[pl.ds(first, rows), span], ref.at[:, span], sems.at[i, k]
            )
            copy.start()
            copies.append(copy)
            first += rows
    for copy in copies:
        copy.wait()


def make_body(Z, X, Y, C):
    def body(inputs, w_query, w_key, w_value, query_gain, key_gain, grad_out):
        T, D = inputs.shape
        nq, nk = w_query.shape[0], w_key.shape[0]
        rows, cols = rotation_constants(Z * X * T // GRID_W)
        DX, DC, PZ = D // X, D // (Y * C), LANES // Z
        sizes = (Z, X, Y, C, T, D)
        tiles = GROUP * T // LANES
        dma = pltpu.SemaphoreType.DMA
        pair = lambda *n: [dma(n), dma(n)]
        vmem = pl.BlockSpec(memory_space=pltpu.VMEM)
        hbm = pl.BlockSpec(memory_space=pltpu.HBM)
        din, gw = pl.pallas_call(
            functools.partial(kernel, sizes),
            out_shape=(
                jax.ShapeDtypeStruct((T, DC), BF16),
                jax.ShapeDtypeStruct((nq + 2 * nk, D), BF16),
            ),
            in_specs=[hbm] * 9,
            out_specs=(vmem, vmem),
            scratch_shapes=[
                pltpu.VMEM((1, HEAD_WIDTH), F32),
                pltpu.VMEM((1, HEAD_WIDTH), F32),
                pltpu.VMEM(rows.shape, F32),
                pltpu.VMEM(cols.shape, F32),
                pltpu.VMEM((nq + 2 * nk, D), BF16),
                pltpu.VMEM((T, D), BF16),
                pltpu.VMEM((Z, T, LANES), BF16),
                pltpu.VMEM((X, T, LANES), BF16),
                pltpu.VMEM((X, T, LANES), BF16),
                pltpu.VMEM((X, tiles, 2 * LANES, LANES), BF16),
                pltpu.VMEM((Z, X, tiles, T, LANES), F32),
                pltpu.VMEM((Z, X, tiles, T, LANES), F32),
                pltpu.VMEM((Z, X, tiles, 3, 1, LANES), F32),
                pltpu.VMEM((Z, X, tiles, 1, LANES), F32),
                pltpu.VMEM((X, tiles, 1, LANES), F32),
                pltpu.VMEM((X, X, 3, tiles, 1, LANES), F32),
                pltpu.VMEM((X, HEAD_WIDTH, GROUP * T), F32),
                pltpu.VMEM((Z, T, LANES), BF16),
                pltpu.VMEM((Z, T, LANES), BF16),
                pltpu.VMEM((X, T, LANES), BF16),
                pltpu.VMEM((X, T, LANES), BF16),
                pltpu.VMEM((X, 2, T, LANES), BF16),
                pltpu.VMEM((X, T, DX), BF16),
                pltpu.VMEM((C, Y, T, DC), BF16),
                pltpu.VMEM((Y, T, DC), BF16),
                pltpu.VMEM((Y, T, DC), BF16),
                pltpu.VMEM((Y, T, DC), BF16),
                pltpu.VMEM((2, LANES, DX), BF16),
                pltpu.VMEM((2, Z, PZ, DX), BF16),
                dma((4 * CHUNKS + 5,)),
                *pair(Z), *pair(X), *pair(X), *pair(X), *pair(X), *pair(Z),
                *pair(X), *pair(X, 2), *pair(Y), *pair(Z, 2), *pair(Z, 2), *pair(X, Z, 2),
            ],
            compiler_params=pltpu.CompilerParams(
                collective_id=0, has_side_effects=True, vmem_limit_bytes=40 * 1024 * 1024
            ),
            name="attention_backward",
        )(
            *[
                pltpu.with_memory_space_constraint(a, pltpu.HBM)
                for a in (
                    inputs, w_query, w_key, w_value, query_gain.reshape(1, -1),
                    key_gain.reshape(1, -1), grad_out, jnp.asarray(rows), jnp.asarray(cols),
                )
            ]
        )
        rest = [jax.ShapeDtypeStruct((n, D), F32) for n in (nq, nk, nk)]
        *grads, din = pl.pallas_call(
            widen,
            out_shape=[*rest, jax.ShapeDtypeStruct((T, DC), BF16)],
            in_specs=[vmem, vmem],
            out_specs=[hbm] * 4,
            scratch_shapes=[pltpu.VMEM((nq + 2 * nk, D), F32), dma((STRIPS + 1, 3))],
            compiler_params=pltpu.CompilerParams(vmem_limit_bytes=16 * 1024 * 1024),
            name="widen",
        )(gw, din)
        return din, *grads

    return body


def solution(mesh):
    Z, X, Y, C = 8, 4, mesh.shape["dp"] // 2, 2
    finer = Mesh(mesh.devices.reshape(Z, X, Y, C), ("z", "x", "y", "c"))
    sp, dp = ("z", "x"), ("y", "c")
    return jax.shard_map(
        make_body(Z, X, Y, C),
        mesh=finer,
        in_specs=(P(sp, None), P(dp, None), P(dp, None), P(dp, None), P(), P(), P(sp, dp)),
        out_specs=(P(sp, dp), P(dp, None), P(dp, None), P(dp, None)),
        check_vma=False,
    )
```

```python
import functools

import jax
import jax.numpy as jnp
import numpy as np
from jax import lax
from jax.experimental import pallas as pl
from jax.experimental.pallas import tpu as pltpu
from jax.sharding import Mesh
from jax.sharding import PartitionSpec as P

HEAD_WIDTH = 64
GRID_W = 64
GROUP = 2
CHUNKS = 2
STRIPS = 4
LANES = 128
MESH = pl.DeviceIdType.MESH
F32 = jnp.float32
BF16 = jnp.bfloat16

norm_eps = 1e-06
axial_base = 10000.0

NT = (((1,), (1,)), ((), ()))
NN = (((1,), (0,)), ((), ()))
TN = (((0,), (0,)), ((), ()))


def dot(a, b, dims):
    return lax.dot_general(a, b, dims, preferred_element_type=F32)


def mark(name):
    pass


def rotation_constants(grid_rows):
    quarter = HEAD_WIDTH // 4
    freqs = axial_base ** (-np.arange(quarter, dtype=np.float64) / quarter)
    by_row = np.arange(grid_rows, dtype=np.float64)[:, None] * freqs
    by_col = np.arange(GRID_W, dtype=np.float64)[:, None] * freqs

    def wide(first, second):
        head = np.concatenate([first, first, second, second], axis=1)
        return np.concatenate([head, head], axis=1)

    none_r, none_c = np.zeros_like(by_row), np.zeros_like(by_col)
    rows = np.stack([wide(np.cos(by_row), none_r), wide(np.sin(by_row), none_r)])
    cols = np.stack([wide(none_c, np.cos(by_col)), wide(none_c, np.sin(by_col))])
    return rows.astype(np.float32), cols.astype(np.float32)


def farthest_first(n):
    return sorted(range(1, n), key=lambda d: -min(d, n - d))


def nearest_first(n):
    return sorted(range(1, n), key=lambda d: min(d, n - d))


def kernel(
    sizes, x_ref, wq_ref, wk_ref, wv_ref, qg_hbm, kg_hbm, do_ref, rows_hbm, cols_hbm,
    din_ref, gw_ref,
    qg_ref, kg_ref, rows_ref, cols_ref, w_all, x_buf, kv_buf, q_buf, do_buf, w_buf, e_buf, dp_buf, stat, cfac, delta, st_buf,
    dqt, dkv_send, dkv_buf, dq_send, dq_buf, g_buf, xin, hp_send, hp_pair, hp_sum, hp_buf, gw_part, gwr_buf,
    load_sem, kv_ss, kv_rs, q_ss, q_rs, do_ss, do_rs, st_ss, st_rs, xin_ss, xin_rs, dkv_ss, dkv_rs,
    dq_ss, dq_rs, g_ss, g_rs, hp_ss, hp_rs, gwr_ss, gwr_rs, agz_ss, agz_rs, agx_ss, agx_rs,
):
    Z, X, Y, C, T, D = sizes
    tiles = GROUP * T // LANES
    DX = D // X
    DC = D // (Y * C)
    PZ = LANES // Z
    z, x, y, c = (lax.axis_index(a) for a in ("z", "x", "y", "c"))

    def on_z(d):
        return {"z": lax.rem(z + d, Z)}

    def on_x(d):
        return {"x": lax.rem(x + d, X)}

    def on_y(d):
        return {"y": lax.rem(y + d, Y)}

    def remote(src, dst, ss, rs, dev):
        return pltpu.make_async_remote_copy(
            src_ref=src, dst_ref=dst, send_sem=ss, recv_sem=rs, device_id=dev, device_id_type=MESH
        )

    barrier = pltpu.get_barrier_semaphore()
    for d in range(1, Z):
        pl.semaphore_signal(barrier, inc=1, device_id=on_z(d), device_id_type=MESH)
    for d in range(1, X):
        pl.semaphore_signal(barrier, inc=1, device_id=on_x(d), device_id_type=MESH)
    for d in range(1, Y):
        pl.semaphore_signal(barrier, inc=1, device_id=on_y(d), device_id_type=MESH)
    pl.semaphore_signal(barrier, inc=1, device_id={"c": 1 - c}, device_id_type=MESH)

    def all_landed(view, ss, rs, dev):
        copy = remote(view, view, ss, rs, dev)
        copy.wait_send()
        copy.wait_recv()

    nq, nk = wq_ref.shape[0], wk_ref.shape[0]
    chunk = D // CHUNKS
    sems = iter(range(load_sem.shape[0]))

    def load(src, dst):
        copy = pltpu.make_async_copy(src, dst, load_sem.at[next(sems)])
        copy.start()
        return copy

    mark("a_issue_loads")
    kv_loads = []
    for i in range(CHUNKS):
        span = pl.ds(i * chunk, chunk)
        kv_loads.append(
            [
                load(x_ref.at[:, span], x_buf.at[:, span]),
                load(wk_ref.at[:, span], w_all.at[pl.ds(nq, nk), span]),
                load(wv_ref.at[:, span], w_all.at[pl.ds(nq + nk, nk), span]),
            ]
        )
    small_loads = [
        load(rows_hbm, rows_ref),
        load(cols_hbm, cols_ref),
        load(qg_hbm, qg_ref),
        load(kg_hbm, kg_ref),
    ]
    late_loads = [load(wq_ref, w_all.at[pl.ds(0, nq)]), load(do_ref, do_buf.at[0])]
    lane = lax.broadcasted_iota(jnp.int32, (T, LANES), 1)
    low = lax.rem(lane, 32) < 16
    head0 = lane < HEAD_WIDTH
    n_rows = T // GRID_W
    first_row = (z * X + x) * n_rows

    def table(k):
        return jnp.concatenate(
            [rows_ref[k, pl.ds(first_row + j, 1), :] + cols_ref[k] for j in range(n_rows)], axis=0
        )

    def turned(v):
        return jnp.where(low, pltpu.roll(v, LANES - 16, 1), pltpu.roll(v, 16, 1))

    def rotate(v):
        return v * cos + turned(v) * sin

    def rotate_back(v):
        return v * cos - turned(v) * sin

    def head_mean(v):
        first = jnp.sum(jnp.where(head0, v, 0.0), axis=1, keepdims=True)
        second = jnp.sum(jnp.where(head0, 0.0, v), axis=1, keepdims=True)
        return jnp.where(head0, first, second) * (1.0 / HEAD_WIDTH)

    mark("b_proj")
    raw = jnp.zeros((T, LANES), F32)
    for i, group in enumerate(kv_loads):
        for copy in group:
            copy.wait()
        span = slice(i * chunk, (i + 1) * chunk)
        raw = raw + dot(x_buf[:, span], w_all[nq:, span], NT)
    kv_raw = raw.astype(BF16).astype(F32)
    for copy in small_loads:
        copy.wait()
    qg = jnp.concatenate([qg_ref[...], qg_ref[...]], axis=1)
    kg = jnp.concatenate([kg_ref[...], kg_ref[...]], axis=1)
    cos = table(0)
    sin = table(1)
    sin = jnp.where(low, -sin, sin)

    k_inv = lax.rsqrt(head_mean(kv_raw * kv_raw) + norm_eps)
    k_hat = kv_raw * k_inv
    kv_buf[0] = jnp.where(head0, rotate(k_hat * kg), kv_raw).astype(BF16)

    mark("c_barrier")
    pl.semaphore_wait(barrier, (Z - 1) + (X - 1) + (Y - 1) + 1)

    mark("d_issue")
    kv_copies, q_copies, do_copies = {}, {}, {}
    for d in nearest_first(Z):
        kv_copies[d] = remote(kv_buf.at[0], kv_buf.at[d], kv_ss.at[0], kv_rs.at[d], on_z(d))
        kv_copies[d].start()
    for copy in late_loads:
        copy.wait()
    q_raw = dot(x_buf[...], w_all[:nq], NT).astype(BF16).astype(F32)
    q_inv = lax.rsqrt(head_mean(q_raw * q_raw) + norm_eps)
    q_hat = q_raw * q_inv
    q_buf[0] = rotate(q_hat * qg).astype(BF16)
    for d in nearest_first(X):
        q_copies[d] = remote(q_buf.at[0], q_buf.at[d], q_ss.at[0], q_rs.at[d], on_x(d))
        q_copies[d].start()
        do_copies[d] = remote(do_buf.at[0], do_buf.at[d], do_ss.at[0], do_rs.at[d], on_x(d))
        do_copies[d].start()

    def send_columns(d):
        cols = pl.multiple_of(lax.rem(x + d, X) * DX, LANES)
        remote(
            x_buf.at[:, pl.ds(cols, DX)], xin.at[d], xin_ss.at[0], xin_rs.at[0], on_x(d)
        ).start()

    near = [d for d in nearest_first(X) if min(d, X - d) == 1]
    for d in near:
        send_columns(d)

    def src_x(d):
        return lax.rem(x + X - d, X)

    def take_queries(d):
        if d:
            mark(f"e_qwait{d}")
            q_copies[d].wait_recv()
            do_copies[d].wait_recv()
        mark(f"f_build{d}")
        q_rows = q_buf[d].astype(F32) * (HEAD_WIDTH**-0.5)
        do_rows = do_buf[d].astype(F32)
        qa = jnp.concatenate(
            [jnp.where(head0, q_rows, 0.0), jnp.where(head0, pltpu.roll(q_rows, HEAD_WIDTH, 1), 0.0)], axis=0
        ).astype(BF16)
        doa = jnp.concatenate(
            [jnp.where(head0, 0.0, pltpu.roll(do_rows, HEAD_WIDTH, 1)), jnp.where(head0, 0.0, do_rows)], axis=0
        ).astype(BF16)
        for t in range(tiles):
            w_buf[d, t, 0:LANES] = qa[t * LANES : (t + 1) * LANES]
            w_buf[d, t, LANES:] = doa[t * LANES : (t + 1) * LANES]

    def take_keys(d):
        if d:
            mark(f"g_kvwait{d}")
            kv_copies[d].wait_recv()

    def forward(d, q):
        kv = kv_buf[d]
        for t in range(tiles):
            both = dot(kv, w_buf[q, t], NT)
            s = both[:, :LANES]
            dp = both[:, LANES:]
            m = jnp.max(s, axis=0, keepdims=True)
            e = jnp.exp(s - m)
            stat[d, q, t, 0] = m
            stat[d, q, t, 1] = jnp.sum(e, axis=0, keepdims=True)
            stat[d, q, t, 2] = jnp.sum(e * dp, axis=0, keepdims=True)
            e_buf[d, q, t] = e
            dp_buf[d, q, t] = dp

    arrivals = []
    zs, xs = [0] + nearest_first(Z), [0] + nearest_first(X)
    order = [("k", 0, 0.0), ("q", 0, 0.0)]
    order += [("k", d, 1.0 + 2.0 * min(d, Z - d) - (d < Z - d) * 0.1) for d in zs[1:]]
    order += [("q", d, 3.5 + 3.0 * (min(d, X - d) - 1) - (d < X - d) * 0.1) for d in xs[1:]]
    keys_in, queries_in = [], []
    for kind, d, _ in sorted(order, key=lambda item: item[2]):
        if kind == "k":
            take_keys(d)
            keys_in.append(d)
            blocks = [(d, q) for q in queries_in]
        else:
            take_queries(d)
            queries_in.append(d)
            blocks = [(k, d) for k in keys_in]
        if blocks:
            mark(f"h_fwd_{kind}{d}")
        for k, q in blocks:
            forward(k, q)

    def merged(parts):
        top = parts[0][0]
        for m, _, _ in parts[1:]:
            top = jnp.maximum(top, m)
        total, weighted = jnp.zeros_like(top), jnp.zeros_like(top)
        for m, l, w in parts:
            f = jnp.exp(m - top)
            total = total + l * f
            weighted = weighted + w * f
        return top, total, weighted

    mark("i_stat")
    for q in range(X):
        parts = [[stat[d, q, :, i] for i in range(3)] for d in range(Z)]
        top, total, weighted = merged(parts)
        st_buf[0, src_x(q), 0] = top + jnp.log(total)
        st_buf[0, src_x(q), 1] = weighted / total
    for d in farthest_first(X):
        remote(st_buf.at[0], st_buf.at[d], st_ss.at[0], st_rs.at[0], on_x(d)).start()
    for d in nearest_first(X):
        if d not in near:
            send_columns(d)
    mark("j_stwait")
    all_landed(st_buf.at[pl.ds(1, X - 1)], st_ss.at[0], st_rs.at[0], on_x(1))
    mark("k_comb")
    for q in range(X):
        at = src_x(q)
        logs = [st_buf[d, at, 0] for d in range(X)]
        top = functools.reduce(jnp.maximum, logs)
        total, weighted = jnp.zeros_like(top), jnp.zeros_like(top)
        for d in range(X):
            f = jnp.exp(logs[d] - top)
            total = total + f
            weighted = weighted + st_buf[d, at, 1] * f
        log_total = top + jnp.log(total)
        delta[q] = weighted / total
        for d in range(Z):
            cfac[d, q] = jnp.exp(stat[d, q, :, 0] - log_total)

    dqt[...] = jnp.zeros_like(dqt)
    dkv_own = dq_own = None

    def as_rows(cols):
        rows = cols.T
        return jnp.concatenate([rows[:T], rows[T:]], axis=1)

    def send_dq(d, cols):
        dq_send[d] = as_rows(cols).astype(BF16)
        remote(
            dq_send.at[d], dq_buf.at[d], dq_ss.at[0], dq_rs.at[0], on_x(X - d)
        ).start()

    for d in farthest_first(Z) + [0]:
        mark(f"l_bwd{d}")
        k_t = kv_buf[d].astype(F32).T[:HEAD_WIDTH].astype(BF16)

        acc = jnp.zeros((T, LANES), F32)
        for q in farthest_first(X) + [0]:
            scores_grad = []
            for t in range(tiles):
                p = e_buf[d, q, t] * cfac[d, q, t]
                ds = (p * (dp_buf[d, q, t] - delta[q, t])).astype(BF16)
                scores_grad.append(ds)
                acc = acc + dot(jnp.concatenate([ds, p.astype(BF16)], axis=1), w_buf[q, t], NN)
            term = dot(k_t, jnp.concatenate(scores_grad, axis=1), NN)
            if d:
                dqt[q] += term
            elif q:
                send_dq(q, dqt[q] + term)
            else:
                dq_own = as_rows(dqt[q] + term)
        if d:
            dkv_send[d] = acc.astype(BF16)
            remote(
                dkv_send.at[d], dkv_buf.at[d], dkv_ss.at[0], dkv_rs.at[0], on_z(Z - d)
            ).start()
        else:
            dkv_own = acc

    def norm_back(grads, normed, inv, gain):
        u = rotate_back(grads) * gain
        return inv * (u - normed * head_mean(u * normed))

    def send_grads(part, value):
        g_buf[0, part] = value
        for d in farthest_first(X):
            remote(
                g_buf.at[0, part], g_buf.at[d, part], g_ss.at[part], g_rs.at[part], on_x(d)
            ).start()

    mark("n_dqwait")
    all_landed(dq_buf.at[pl.ds(1, X - 1)], dq_ss.at[0], dq_rs.at[0], on_x(1))
    for d in range(1, X):
        dq_own = dq_own + dq_buf[d].astype(F32)
    mark("n_normq")
    grad_q = norm_back(dq_own * (HEAD_WIDTH**-0.5), q_hat, q_inv, qg).astype(BF16)
    send_grads(0, grad_q)
    mark("o_dkvwait")
    all_landed(dkv_buf.at[pl.ds(1, Z - 1)], dkv_ss.at[0], dkv_rs.at[0], on_z(1))
    for d in range(1, Z):
        dkv_own = dkv_own + dkv_buf[d].astype(F32)
    mark("p_normk")
    grad_k = norm_back(jnp.where(head0, dkv_own, 0.0), k_hat, k_inv, kg)
    grad_kv = jnp.where(head0, grad_k, dkv_own).astype(BF16)
    send_grads(1, grad_kv)

    mark("q_hp")
    g = jnp.concatenate([grad_q, grad_kv], axis=1)
    for j in range(Y):
        two = dot(g, w_all[:, j * C * DC : (j + 1) * C * DC], NN).astype(BF16)
        for k in range(C):
            hp_send[k, j] = two[:, k * DC : (k + 1) * DC]
    pair_copy = remote(hp_send.at[1 - c], hp_pair, hp_ss.at[0], hp_rs.at[0], {"c": 1 - c})
    pair_copy.start()

    def send_parts():
        mark("q_pair")
        pair_copy.wait()
        for j in range(Y):
            hp_sum[j] = (hp_send[c, j].astype(F32) + hp_pair[j].astype(F32)).astype(BF16)
        for d in farthest_first(Y):
            remote(
                hp_sum.at[lax.rem(y + d, Y)], hp_buf.at[d], hp_ss.at[1], hp_rs.at[1], on_y(d)
            ).start()

    cols = pl.multiple_of(x * DX, LANES)
    agz_copies = {}

    def multiply(part):
        gw = dot(g_buf[0, part], x_buf[:, pl.ds(cols, DX)], TN)
        all_landed(g_buf.at[pl.ds(1, X - 1), part], g_ss.at[part], g_rs.at[part], on_x(1))
        if not part:
            all_landed(xin.at[pl.ds(1, X - 1)], xin_ss.at[0], xin_rs.at[0], on_x(1))
        for d in range(1, X):
            gw = gw + dot(g_buf[d, part], xin[d], TN)
        gw_part[part] = gw.astype(BF16)
        for d in farthest_first(Z):
            rows = pl.multiple_of(lax.rem(z + d, Z) * PZ, PZ)
            remote(
                gw_part.at[part, pl.ds(rows, PZ)], gwr_buf.at[part, d],
                gwr_ss.at[part], gwr_rs.at[part], on_z(d),
            ).start()

    def region(part, dz):
        rows = pl.multiple_of(part * LANES + lax.rem(z + Z - dz, Z) * PZ, PZ)
        return gw_ref.at[pl.ds(rows, PZ), pl.ds(cols, DX)]

    def pass_on(part, dz):
        block = region(part, dz)
        for d in farthest_first(X):
            remote(block, block, agx_ss.at[0], agx_rs.at[0], on_x(d)).start()

    def add_up(part):
        my_rows = pl.multiple_of(z * PZ, PZ)
        piece = gw_part[part, pl.ds(my_rows, PZ), :].astype(F32)
        all_landed(gwr_buf.at[part, pl.ds(1, Z - 1)], gwr_ss.at[part], gwr_rs.at[part], on_z(1))
        for d in range(1, Z):
            piece = piece + gwr_buf[part, d].astype(F32)
        gw_ref[
            pl.ds(pl.multiple_of(part * LANES + my_rows, PZ), PZ),
            pl.ds(cols, DX),
        ] = piece.astype(BF16)
        own = region(part, 0)
        for d in nearest_first(Z):
            agz_copies[part, d] = remote(own, own, agz_ss.at[part], agz_rs.at[d, part], on_z(d))
            agz_copies[part, d].start()
        pass_on(part, 0)

    for part in range(2):
        mark(f"r_gw{part}")
        multiply(part)
    send_parts()
    for part in range(2):
        mark(f"s_gwrwait{part}")
        add_up(part)
    for part in range(2):
        mark(f"t_agz{part}")
        for dz in nearest_first(Z):
            agz_copies[part, dz].wait_recv()
            pass_on(part, dz)
    mark("u_hpwait")
    din = hp_sum[y].astype(F32)
    all_landed(hp_buf.at[pl.ds(1, Y - 1)], hp_ss.at[1], hp_rs.at[1], on_y(1))
    for d in range(1, Y):
        din = din + hp_buf[d].astype(F32)
    din_ref[...] = din.astype(BF16)
    mark("v_agxwait")
    all_landed(gw_ref.at[:, pl.ds(0, (X - 1) * DX)], agx_ss.at[0], agx_rs.at[0], on_x(1))
    view = kv_buf.at[pl.ds(1, Z - 1)]
    remote(view, view, kv_ss.at[0], kv_rs.at[0], on_z(1)).wait_send()
    for buf, ss, rs in ((q_buf, q_ss, q_rs), (do_buf, do_ss, do_rs)):
        view = buf.at[pl.ds(1, X - 1)]
        remote(view, view, ss.at[0], rs.at[0], on_x(1)).wait_send()
    for part in range(2):
        view = gwr_buf.at[part, pl.ds(1, Z - 1)]
        remote(view, view, agz_ss.at[part], agz_rs.at[0, part], on_z(1)).wait_send()
    mark(None)


def widen(gw_ref, din_ref, *refs):
    *grad_refs, din_out, wide, sems = refs
    last = pltpu.make_async_copy(din_ref, din_out, sems.at[STRIPS, 0])
    last.start()
    copies = [last]
    strip = gw_ref.shape[1] // STRIPS
    for i in range(STRIPS):
        span = pl.ds(i * strip, strip)
        wide[:, span] = gw_ref[:, span].astype(F32)
        first = 0
        for k, ref in enumerate(grad_refs):
            rows = ref.shape[0]
            copy = pltpu.make_async_copy(
                wide.at[pl.ds(first, rows), span], ref.at[:, span], sems.at[i, k]
            )
            copy.start()
            copies.append(copy)
            first += rows
    for copy in copies:
        copy.wait()


def make_body(Z, X, Y, C):
    def body(inputs, w_query, w_key, w_value, query_gain, key_gain, grad_out):
        T, D = inputs.shape
        nq, nk = w_query.shape[0], w_key.shape[0]
        rows, cols = rotation_constants(Z * X * T // GRID_W)
        DX, DC, PZ = D // X, D // (Y * C), LANES // Z
        sizes = (Z, X, Y, C, T, D)
        tiles = GROUP * T // LANES
        dma = pltpu.SemaphoreType.DMA
        pair = lambda *n: [dma(n), dma(n)]
        vmem = pl.BlockSpec(memory_space=pltpu.VMEM)
        hbm = pl.BlockSpec(memory_space=pltpu.HBM)
        din, gw = pl.pallas_call(
            functools.partial(kernel, sizes),
            out_shape=(
                jax.ShapeDtypeStruct((T, DC), BF16),
                jax.ShapeDtypeStruct((nq + 2 * nk, D), BF16),
            ),
            in_specs=[hbm] * 9,
            out_specs=(vmem, vmem),
            scratch_shapes=[
                pltpu.VMEM((1, HEAD_WIDTH), F32),
                pltpu.VMEM((1, HEAD_WIDTH), F32),
                pltpu.VMEM(rows.shape, F32),
                pltpu.VMEM(cols.shape, F32),
                pltpu.VMEM((nq + 2 * nk, D), BF16),
                pltpu.VMEM((T, D), BF16),
                pltpu.VMEM((Z, T, LANES), BF16),
                pltpu.VMEM((X, T, LANES), BF16),
                pltpu.VMEM((X, T, LANES), BF16),
                pltpu.VMEM((X, tiles, 2 * LANES, LANES), BF16),
                pltpu.VMEM((Z, X, tiles, T, LANES), F32),
                pltpu.VMEM((Z, X, tiles, T, LANES), F32),
                pltpu.VMEM((Z, X, tiles, 3, 1, LANES), F32),
                pltpu.VMEM((Z, X, tiles, 1, LANES), F32),
                pltpu.VMEM((X, tiles, 1, LANES), F32),
                pltpu.VMEM((X, X, 2, tiles, 1, LANES), F32),
                pltpu.VMEM((X, HEAD_WIDTH, GROUP * T), F32),
                pltpu.VMEM((Z, T, LANES), BF16),
                pltpu.VMEM((Z, T, LANES), BF16),
                pltpu.VMEM((X, T, LANES), BF16),
                pltpu.VMEM((X, T, LANES), BF16),
                pltpu.VMEM((X, 2, T, LANES), BF16),
                pltpu.VMEM((X, T, DX), BF16),
                pltpu.VMEM((C, Y, T, DC), BF16),
                pltpu.VMEM((Y, T, DC), BF16),
                pltpu.VMEM((Y, T, DC), BF16),
                pltpu.VMEM((Y, T, DC), BF16),
                pltpu.VMEM((2, LANES, DX), BF16),
                pltpu.VMEM((2, Z, PZ, DX), BF16),
                dma((3 * CHUNKS + 6,)),
                dma((1,)), dma((Z,)), dma((1,)), dma((X,)), dma((1,)), dma((X,)), *pair(1), *pair(1), *pair(1),
                *pair(1), *pair(2), *pair(2), *pair(2), dma((2,)), dma((Z, 2)), *pair(1),
            ],
            compiler_params=pltpu.CompilerParams(
                collective_id=0, has_side_effects=True, vmem_limit_bytes=40 * 1024 * 1024
            ),
            name="attention_backward",
        )(
            *[
                pltpu.with_memory_space_constraint(a, pltpu.HBM)
                for a in (
                    inputs, w_query, w_key, w_value, query_gain.reshape(1, -1),
                    key_gain.reshape(1, -1), grad_out, jnp.asarray(rows), jnp.asarray(cols),
                )
            ]
        )
        rest = [jax.ShapeDtypeStruct((n, D), F32) for n in (nq, nk, nk)]
        *grads, din = pl.pallas_call(
            widen,
            out_shape=[*rest, jax.ShapeDtypeStruct((T, DC), BF16)],
            in_specs=[vmem, vmem],
            out_specs=[hbm] * 4,
            scratch_shapes=[pltpu.VMEM((nq + 2 * nk, D), F32), dma((STRIPS + 1, 3))],
            compiler_params=pltpu.CompilerParams(vmem_limit_bytes=16 * 1024 * 1024),
            name="widen",
        )(gw, din)
        return din, *grads

    return body


def solution(mesh):
    Z, X, Y, C = 8, 4, mesh.shape["dp"] // 2, 2
    finer = Mesh(mesh.devices.reshape(Z, X, Y, C), ("z", "x", "y", "c"))
    sp, dp = ("z", "x"), ("y", "c")
    return jax.shard_map(
        make_body(Z, X, Y, C),
        mesh=finer,
        in_specs=(P(sp, None), P(dp, None), P(dp, None), P(dp, None), P(), P(), P(sp, dp)),
        out_specs=(P(sp, dp), P(dp, None), P(dp, None), P(dp, None)),
        check_vma=False,
    )
```

```python
import functools

import jax
import jax.numpy as jnp
import numpy as np
from jax import lax
from jax.experimental import pallas as pl
from jax.experimental.pallas import tpu as pltpu
from jax.sharding import Mesh
from jax.sharding import PartitionSpec as P

HEAD_WIDTH = 64
GRID_W = 64
GROUP = 2
CHUNKS = 2
STRIPS = 4
LANES = 128
MESH = pl.DeviceIdType.MESH
F32 = jnp.float32
BF16 = jnp.bfloat16

norm_eps = 1e-06
axial_base = 10000.0

NT = (((1,), (1,)), ((), ()))
NN = (((1,), (0,)), ((), ()))
TN = (((0,), (0,)), ((), ()))


def dot(a, b, dims):
    return lax.dot_general(a, b, dims, preferred_element_type=F32)


def mark(name):
    pass


def rotation_constants(grid_rows):
    quarter = HEAD_WIDTH // 4
    freqs = axial_base ** (-np.arange(quarter, dtype=np.float64) / quarter)
    by_row = np.arange(grid_rows, dtype=np.float64)[:, None] * freqs
    by_col = np.arange(GRID_W, dtype=np.float64)[:, None] * freqs

    def wide(first, second):
        head = np.concatenate([first, first, second, second], axis=1)
        return np.concatenate([head, head], axis=1)

    none_r, none_c = np.zeros_like(by_row), np.zeros_like(by_col)
    rows = np.stack([wide(np.cos(by_row), none_r), wide(np.sin(by_row), none_r)])
    cols = np.stack([wide(none_c, np.cos(by_col)), wide(none_c, np.sin(by_col))])
    return rows.astype(np.float32), cols.astype(np.float32)


def farthest_first(n):
    return sorted(range(1, n), key=lambda d: -min(d, n - d))


def nearest_first(n):
    return sorted(range(1, n), key=lambda d: min(d, n - d))


def kernel(
    sizes, x_ref, wq_ref, wk_ref, wv_ref, qg_hbm, kg_hbm, do_ref, rows_hbm, cols_hbm,
    din_ref, gw_ref,
    qg_ref, kg_ref, rows_ref, cols_ref, w_all, x_buf, kv_buf, q_buf, do_buf, w_buf, e_buf, dp_buf, stat, cfac, delta, st_buf,
    dqt, dkv_send, dkv_buf, dq_send, dq_buf, g_buf, xin, hp_send, hp_pair, hp_sum, hp_buf, gw_part, gwr_buf,
    load_sem, kv_ss, kv_rs, q_ss, q_rs, do_ss, do_rs, st_ss, st_rs, xin_ss, xin_rs, dkv_ss, dkv_rs,
    dq_ss, dq_rs, g_ss, g_rs, hp_ss, hp_rs, gwr_ss, gwr_rs, agz_ss, agz_rs, agx_ss, agx_rs,
):
    Z, X, Y, C, T, D = sizes
    tiles = GROUP * T // LANES
    DX = D // X
    DC = D // (Y * C)
    PZ = LANES // Z
    z, x, y, c = (lax.axis_index(a) for a in ("z", "x", "y", "c"))

    def on_z(d):
        return {"z": lax.rem(z + d, Z)}

    def on_x(d):
        return {"x": lax.rem(x + d, X)}

    def on_y(d):
        return {"y": lax.rem(y + d, Y)}

    def remote(src, dst, ss, rs, dev):
        return pltpu.make_async_remote_copy(
            src_ref=src, dst_ref=dst, send_sem=ss, recv_sem=rs, device_id=dev, device_id_type=MESH
        )

    barrier = pltpu.get_barrier_semaphore()
    for d in range(1, Z):
        pl.semaphore_signal(barrier, inc=1, device_id=on_z(d), device_id_type=MESH)
    for d in range(1, X):
        pl.semaphore_signal(barrier, inc=1, device_id=on_x(d), device_id_type=MESH)
    for d in range(1, Y):
        pl.semaphore_signal(barrier, inc=1, device_id=on_y(d), device_id_type=MESH)
    pl.semaphore_signal(barrier, inc=1, device_id={"c": 1 - c}, device_id_type=MESH)

    def all_landed(view, ss, rs, dev):
        copy = remote(view, view, ss, rs, dev)
        copy.wait_send()
        copy.wait_recv()

    nq, nk = wq_ref.shape[0], wk_ref.shape[0]
    chunk = D // CHUNKS
    sems = iter(range(load_sem.shape[0]))

    def load(src, dst):
        copy = pltpu.make_async_copy(src, dst, load_sem.at[next(sems)])
        copy.start()
        return copy

    mark("a_issue_loads")
    kv_loads = []
    for i in range(CHUNKS):
        span = pl.ds(i * chunk, chunk)
        kv_loads.append(
            [
                load(x_ref.at[:, span], x_buf.at[:, span]),
                load(wk_ref.at[:, span], w_all.at[pl.ds(nq, nk), span]),
                load(wv_ref.at[:, span], w_all.at[pl.ds(nq + nk, nk), span]),
            ]
        )
    small_loads = [
        load(rows_hbm, rows_ref),
        load(cols_hbm, cols_ref),
        load(qg_hbm, qg_ref),
        load(kg_hbm, kg_ref),
    ]
    late_loads = [load(wq_ref, w_all.at[pl.ds(0, nq)]), load(do_ref, do_buf.at[0])]
    lane = lax.broadcasted_iota(jnp.int32, (T, LANES), 1)
    low = lax.rem(lane, 32) < 16
    head0 = lane < HEAD_WIDTH
    n_rows = T // GRID_W
    first_row = (z * X + x) * n_rows

    def table(k):
        return jnp.concatenate(
            [rows_ref[k, pl.ds(first_row + j, 1), :] + cols_ref[k] for j in range(n_rows)], axis=0
        )

    def turned(v):
        return jnp.where(low, pltpu.roll(v, LANES - 16, 1), pltpu.roll(v, 16, 1))

    def rotate(v):
        return v * cos + turned(v) * sin

    def rotate_back(v):
        return v * cos - turned(v) * sin

    def head_mean(v):
        first = jnp.sum(jnp.where(head0, v, 0.0), axis=1, keepdims=True)
        second = jnp.sum(jnp.where(head0, 0.0, v), axis=1, keepdims=True)
        return jnp.where(head0, first, second) * (1.0 / HEAD_WIDTH)

    mark("b_proj")
    raw = jnp.zeros((T, LANES), F32)
    for i, group in enumerate(kv_loads):
        for copy in group:
            copy.wait()
        span = slice(i * chunk, (i + 1) * chunk)
        raw = raw + dot(x_buf[:, span], w_all[nq:, span], NT)
    kv_raw = raw.astype(BF16).astype(F32)
    for copy in small_loads:
        copy.wait()
    qg = jnp.concatenate([qg_ref[...], qg_ref[...]], axis=1)
    kg = jnp.concatenate([kg_ref[...], kg_ref[...]], axis=1)
    cos = table(0)
    sin = table(1)
    sin = jnp.where(low, -sin, sin)

    k_inv = lax.rsqrt(head_mean(kv_raw * kv_raw) + norm_eps)
    k_hat = kv_raw * k_inv
    kv_buf[0] = jnp.where(head0, rotate(k_hat * kg), kv_raw).astype(BF16)

    mark("c_barrier")
    pl.semaphore_wait(barrier, (Z - 1) + (X - 1) + (Y - 1) + 1)

    mark("d_issue")
    kv_copies, q_copies, do_copies = {}, {}, {}
    for d in nearest_first(Z):
        kv_copies[d] = remote(kv_buf.at[0], kv_buf.at[d], kv_ss.at[0], kv_rs.at[d], on_z(d))
        kv_copies[d].start()
    late_loads[1].wait()
    for d in nearest_first(X):
        do_copies[d] = remote(do_buf.at[0], do_buf.at[d], do_ss.at[0], do_rs.at[d], on_x(d))
        do_copies[d].start()
    late_loads[0].wait()
    q_raw = dot(x_buf[...], w_all[:nq], NT).astype(BF16).astype(F32)
    q_inv = lax.rsqrt(head_mean(q_raw * q_raw) + norm_eps)
    q_hat = q_raw * q_inv
    q_buf[0] = rotate(q_hat * qg).astype(BF16)
    for d in nearest_first(X):
        q_copies[d] = remote(q_buf.at[0], q_buf.at[d], q_ss.at[0], q_rs.at[d], on_x(d))
        q_copies[d].start()

    def send_columns(d):
        cols = pl.multiple_of(lax.rem(x + d, X) * DX, LANES)
        remote(
            x_buf.at[:, pl.ds(cols, DX)], xin.at[d], xin_ss.at[0], xin_rs.at[0], on_x(d)
        ).start()

    near = [d for d in nearest_first(X) if min(d, X - d) == 1]
    for d in near:
        send_columns(d)

    def src_x(d):
        return lax.rem(x + X - d, X)

    def take_queries(d):
        if d:
            mark(f"e_qwait{d}")
            q_copies[d].wait_recv()
            do_copies[d].wait_recv()
        mark(f"f_build{d}")
        q_rows = q_buf[d].astype(F32) * (HEAD_WIDTH**-0.5)
        do_rows = do_buf[d].astype(F32)
        qa = jnp.concatenate(
            [jnp.where(head0, q_rows, 0.0), jnp.where(head0, pltpu.roll(q_rows, HEAD_WIDTH, 1), 0.0)], axis=0
        ).astype(BF16)
        doa = jnp.concatenate(
            [jnp.where(head0, 0.0, pltpu.roll(do_rows, HEAD_WIDTH, 1)), jnp.where(head0, 0.0, do_rows)], axis=0
        ).astype(BF16)
        for t in range(tiles):
            w_buf[d, t, 0:LANES] = qa[t * LANES : (t + 1) * LANES]
            w_buf[d, t, LANES:] = doa[t * LANES : (t + 1) * LANES]

    def take_keys(d):
        if d:
            mark(f"g_kvwait{d}")
            kv_copies[d].wait_recv()

    def forward(d, q):
        kv = kv_buf[d]
        for t in range(tiles):
            both = dot(kv, w_buf[q, t], NT)
            s = both[:, :LANES]
            dp = both[:, LANES:]
            m = jnp.max(s, axis=0, keepdims=True)
            e = jnp.exp(s - m)
            stat[d, q, t, 0] = m
            stat[d, q, t, 1] = jnp.sum(e, axis=0, keepdims=True)
            stat[d, q, t, 2] = jnp.sum(e * dp, axis=0, keepdims=True)
            e_buf[d, q, t] = e
            dp_buf[d, q, t] = dp

    arrivals = []
    zs, xs = [0] + nearest_first(Z), [0] + nearest_first(X)
    order = [("k", 0, 0.0), ("q", 0, 0.0)]
    order += [("k", d, 1.0 + 2.0 * min(d, Z - d) - (d < Z - d) * 0.1) for d in zs[1:]]
    order += [("q", d, 3.5 + 3.0 * (min(d, X - d) - 1) - (d < X - d) * 0.1) for d in xs[1:]]
    keys_in, queries_in = [], []
    for kind, d, _ in sorted(order, key=lambda item: item[2]):
        if kind == "k":
            take_keys(d)
            keys_in.append(d)
            blocks = [(d, q) for q in queries_in]
        else:
            take_queries(d)
            queries_in.append(d)
            blocks = [(k, d) for k in keys_in]
        if blocks:
            mark(f"h_fwd_{kind}{d}")
        for k, q in blocks:
            forward(k, q)

    def merged(parts):
        top = parts[0][0]
        for m, _, _ in parts[1:]:
            top = jnp.maximum(top, m)
        total, weighted = jnp.zeros_like(top), jnp.zeros_like(top)
        for m, l, w in parts:
            f = jnp.exp(m - top)
            total = total + l * f
            weighted = weighted + w * f
        return top, total, weighted

    mark("i_stat")
    for q in range(X):
        parts = [[stat[d, q, :, i] for i in range(3)] for d in range(Z)]
        top, total, weighted = merged(parts)
        st_buf[0, src_x(q), 0] = top + jnp.log(total)
        st_buf[0, src_x(q), 1] = weighted / total
    for d in farthest_first(X):
        remote(st_buf.at[0], st_buf.at[d], st_ss.at[0], st_rs.at[0], on_x(d)).start()
    for d in nearest_first(X):
        if d not in near:
            send_columns(d)
    mark("j_stwait")
    all_landed(st_buf.at[pl.ds(1, X - 1)], st_ss.at[0], st_rs.at[0], on_x(1))
    mark("k_comb")
    for q in range(X):
        at = src_x(q)
        logs = [st_buf[d, at, 0] for d in range(X)]
        top = functools.reduce(jnp.maximum, logs)
        total, weighted = jnp.zeros_like(top), jnp.zeros_like(top)
        for d in range(X):
            f = jnp.exp(logs[d] - top)
            total = total + f
            weighted = weighted + st_buf[d, at, 1] * f
        log_total = top + jnp.log(total)
        delta[q] = weighted / total
        for d in range(Z):
            cfac[d, q] = jnp.exp(stat[d, q, :, 0] - log_total)

    dqt[...] = jnp.zeros_like(dqt)
    dkv_own = dq_own = None

    def as_rows(cols):
        rows = cols.T
        return jnp.concatenate([rows[:T], rows[T:]], axis=1)

    def send_dq(d, cols):
        dq_send[d] = as_rows(cols).astype(BF16)
        remote(
            dq_send.at[d], dq_buf.at[d], dq_ss.at[0], dq_rs.at[0], on_x(X - d)
        ).start()

    for d in farthest_first(Z) + [0]:
        mark(f"l_bwd{d}")
        k_t = kv_buf[d].astype(F32).T[:HEAD_WIDTH].astype(BF16)

        acc = jnp.zeros((T, LANES), F32)
        for q in farthest_first(X) + [0]:
            scores_grad = []
            for t in range(tiles):
                p = e_buf[d, q, t] * cfac[d, q, t]
                ds = (p * (dp_buf[d, q, t] - delta[q, t])).astype(BF16)
                scores_grad.append(ds)
                acc = acc + dot(jnp.concatenate([ds, p.astype(BF16)], axis=1), w_buf[q, t], NN)
            term = dot(k_t, jnp.concatenate(scores_grad, axis=1), NN)
            dqt[q] += term
        if d:
            dkv_send[d] = acc.astype(BF16)
            remote(
                dkv_send.at[d], dkv_buf.at[d], dkv_ss.at[0], dkv_rs.at[0], on_z(Z - d)
            ).start()
        else:
            dkv_own = acc
    for q in farthest_first(X):
        send_dq(q, dqt[q])
    dq_own = as_rows(dqt[0])

    def norm_back(grads, normed, inv, gain):
        u = rotate_back(grads) * gain
        return inv * (u - normed * head_mean(u * normed))

    def send_grads(part, value):
        g_buf[0, part] = value
        for d in farthest_first(X):
            remote(
                g_buf.at[0, part], g_buf.at[d, part], g_ss.at[part], g_rs.at[part], on_x(d)
            ).start()

    mark("n_dqwait")
    all_landed(dq_buf.at[pl.ds(1, X - 1)], dq_ss.at[0], dq_rs.at[0], on_x(1))
    for d in range(1, X):
        dq_own = dq_own + dq_buf[d].astype(F32)
    mark("n_normq")
    grad_q = norm_back(dq_own * (HEAD_WIDTH**-0.5), q_hat, q_inv, qg).astype(BF16)
    send_grads(0, grad_q)
    mark("o_dkvwait")
    all_landed(dkv_buf.at[pl.ds(1, Z - 1)], dkv_ss.at[0], dkv_rs.at[0], on_z(1))
    for d in range(1, Z):
        dkv_own = dkv_own + dkv_buf[d].astype(F32)
    mark("p_normk")
    grad_k = norm_back(jnp.where(head0, dkv_own, 0.0), k_hat, k_inv, kg)
    grad_kv = jnp.where(head0, grad_k, dkv_own).astype(BF16)
    send_grads(1, grad_kv)

    mark("q_hp")
    g = jnp.concatenate([grad_q, grad_kv], axis=1)
    for j in range(Y):
        two = dot(g, w_all[:, j * C * DC : (j + 1) * C * DC], NN).astype(BF16)
        for k in range(C):
            hp_send[k, j] = two[:, k * DC : (k + 1) * DC]
    pair_copy = remote(hp_send.at[1 - c], hp_pair, hp_ss.at[0], hp_rs.at[0], {"c": 1 - c})
    pair_copy.start()

    def send_parts():
        mark("q_pair")
        pair_copy.wait()
        for j in range(Y):
            hp_sum[j] = (hp_send[c, j].astype(F32) + hp_pair[j].astype(F32)).astype(BF16)
        for d in farthest_first(Y):
            remote(
                hp_sum.at[lax.rem(y + d, Y)], hp_buf.at[d], hp_ss.at[1], hp_rs.at[1], on_y(d)
            ).start()

    cols = pl.multiple_of(x * DX, LANES)
    agz_copies = {}

    def multiply(part):
        gw = dot(g_buf[0, part], x_buf[:, pl.ds(cols, DX)], TN)
        all_landed(g_buf.at[pl.ds(1, X - 1), part], g_ss.at[part], g_rs.at[part], on_x(1))
        if not part:
            all_landed(xin.at[pl.ds(1, X - 1)], xin_ss.at[0], xin_rs.at[0], on_x(1))
        for d in range(1, X):
            gw = gw + dot(g_buf[d, part], xin[d], TN)
        gw_part[part] = gw.astype(BF16)
        for d in farthest_first(Z):
            rows = pl.multiple_of(lax.rem(z + d, Z) * PZ, PZ)
            remote(
                gw_part.at[part, pl.ds(rows, PZ)], gwr_buf.at[part, d],
                gwr_ss.at[part], gwr_rs.at[part], on_z(d),
            ).start()

    def region(part, dz):
        rows = pl.multiple_of(part * LANES + lax.rem(z + Z - dz, Z) * PZ, PZ)
        return gw_ref.at[pl.ds(rows, PZ), pl.ds(cols, DX)]

    def pass_on(part, dz):
        block = region(part, dz)
        for d in farthest_first(X):
            remote(block, block, agx_ss.at[0], agx_rs.at[0], on_x(d)).start()

    def add_up(part):
        my_rows = pl.multiple_of(z * PZ, PZ)
        piece = gw_part[part, pl.ds(my_rows, PZ), :].astype(F32)
        all_landed(gwr_buf.at[part, pl.ds(1, Z - 1)], gwr_ss.at[part], gwr_rs.at[part], on_z(1))
        for d in range(1, Z):
            piece = piece + gwr_buf[part, d].astype(F32)
        gw_ref[
            pl.ds(pl.multiple_of(part * LANES + my_rows, PZ), PZ),
            pl.ds(cols, DX),
        ] = piece.astype(BF16)
        own = region(part, 0)
        for d in nearest_first(Z):
            agz_copies[part, d] = remote(own, own, agz_ss.at[part], agz_rs.at[d, part], on_z(d))
            agz_copies[part, d].start()
        pass_on(part, 0)

    for part in range(2):
        mark(f"r_gw{part}")
        multiply(part)
    send_parts()
    for part in range(2):
        mark(f"s_gwrwait{part}")
        add_up(part)
    for part in range(2):
        mark(f"t_agz{part}")
        for dz in nearest_first(Z):
            agz_copies[part, dz].wait_recv()
            pass_on(part, dz)
    mark("u_hpwait")
    din = hp_sum[y].astype(F32)
    all_landed(hp_buf.at[pl.ds(1, Y - 1)], hp_ss.at[1], hp_rs.at[1], on_y(1))
    for d in range(1, Y):
        din = din + hp_buf[d].astype(F32)
    din_ref[...] = din.astype(BF16)
    mark("v_agxwait")
    all_landed(gw_ref.at[:, pl.ds(0, (X - 1) * DX)], agx_ss.at[0], agx_rs.at[0], on_x(1))
    view = kv_buf.at[pl.ds(1, Z - 1)]
    remote(view, view, kv_ss.at[0], kv_rs.at[0], on_z(1)).wait_send()
    for buf, ss, rs in ((q_buf, q_ss, q_rs), (do_buf, do_ss, do_rs)):
        view = buf.at[pl.ds(1, X - 1)]
        remote(view, view, ss.at[0], rs.at[0], on_x(1)).wait_send()
    for part in range(2):
        view = gwr_buf.at[part, pl.ds(1, Z - 1)]
        remote(view, view, agz_ss.at[part], agz_rs.at[0, part], on_z(1)).wait_send()
    mark(None)


def widen(gw_ref, din_ref, *refs):
    *grad_refs, din_out, wide, sems = refs
    last = pltpu.make_async_copy(din_ref, din_out, sems.at[STRIPS, 0])
    last.start()
    copies = [last]
    strip = gw_ref.shape[1] // STRIPS
    for i in range(STRIPS):
        span = pl.ds(i * strip, strip)
        wide[:, span] = gw_ref[:, span].astype(F32)
        first = 0
        for k, ref in enumerate(grad_refs):
            rows = ref.shape[0]
            copy = pltpu.make_async_copy(
                wide.at[pl.ds(first, rows), span], ref.at[:, span], sems.at[i, k]
            )
            copy.start()
            copies.append(copy)
            first += rows
    for copy in copies:
        copy.wait()


def make_body(Z, X, Y, C):
    def body(inputs, w_query, w_key, w_value, query_gain, key_gain, grad_out):
        T, D = inputs.shape
        nq, nk = w_query.shape[0], w_key.shape[0]
        rows, cols = rotation_constants(Z * X * T // GRID_W)
        DX, DC, PZ = D // X, D // (Y * C), LANES // Z
        sizes = (Z, X, Y, C, T, D)
        tiles = GROUP * T // LANES
        dma = pltpu.SemaphoreType.DMA
        pair = lambda *n: [dma(n), dma(n)]
        vmem = pl.BlockSpec(memory_space=pltpu.VMEM)
        hbm = pl.BlockSpec(memory_space=pltpu.HBM)
        din, gw = pl.pallas_call(
            functools.partial(kernel, sizes),
            out_shape=(
                jax.ShapeDtypeStruct((T, DC), BF16),
                jax.ShapeDtypeStruct((nq + 2 * nk, D), BF16),
            ),
            in_specs=[hbm] * 9,
            out_specs=(vmem, vmem),
            scratch_shapes=[
                pltpu.VMEM((1, HEAD_WIDTH), F32),
                pltpu.VMEM((1, HEAD_WIDTH), F32),
                pltpu.VMEM(rows.shape, F32),
                pltpu.VMEM(cols.shape, F32),
                pltpu.VMEM((nq + 2 * nk, D), BF16),
                pltpu.VMEM((T, D), BF16),
                pltpu.VMEM((Z, T, LANES), BF16),
                pltpu.VMEM((X, T, LANES), BF16),
                pltpu.VMEM((X, T, LANES), BF16),
                pltpu.VMEM((X, tiles, 2 * LANES, LANES), BF16),
                pltpu.VMEM((Z, X, tiles, T, LANES), F32),
                pltpu.VMEM((Z, X, tiles, T, LANES), F32),
                pltpu.VMEM((Z, X, tiles, 3, 1, LANES), F32),
                pltpu.VMEM((Z, X, tiles, 1, LANES), F32),
                pltpu.VMEM((X, tiles, 1, LANES), F32),
                pltpu.VMEM((X, X, 2, tiles, 1, LANES), F32),
                pltpu.VMEM((X, HEAD_WIDTH, GROUP * T), F32),
                pltpu.VMEM((Z, T, LANES), BF16),
                pltpu.VMEM((Z, T, LANES), BF16),
                pltpu.VMEM((X, T, LANES), BF16),
                pltpu.VMEM((X, T, LANES), BF16),
                pltpu.VMEM((X, 2, T, LANES), BF16),
                pltpu.VMEM((X, T, DX), BF16),
                pltpu.VMEM((C, Y, T, DC), BF16),
                pltpu.VMEM((Y, T, DC), BF16),
                pltpu.VMEM((Y, T, DC), BF16),
                pltpu.VMEM((Y, T, DC), BF16),
                pltpu.VMEM((2, LANES, DX), BF16),
                pltpu.VMEM((2, Z, PZ, DX), BF16),
                dma((3 * CHUNKS + 6,)),
                dma((1,)), dma((Z,)), dma((1,)), dma((X,)), dma((1,)), dma((X,)), *pair(1), *pair(1), *pair(1),
                *pair(1), *pair(2), *pair(2), *pair(2), dma((2,)), dma((Z, 2)), *pair(1),
            ],
            compiler_params=pltpu.CompilerParams(
                collective_id=0, has_side_effects=True, vmem_limit_bytes=40 * 1024 * 1024
            ),
            name="attention_backward",
        )(
            *[
                pltpu.with_memory_space_constraint(a, pltpu.HBM)
                for a in (
                    inputs, w_query, w_key, w_value, query_gain.reshape(1, -1),
                    key_gain.reshape(1, -1), grad_out, jnp.asarray(rows), jnp.asarray(cols),
                )
            ]
        )
        rest = [jax.ShapeDtypeStruct((n, D), F32) for n in (nq, nk, nk)]
        *grads, din = pl.pallas_call(
            widen,
            out_shape=[*rest, jax.ShapeDtypeStruct((T, DC), BF16)],
            in_specs=[vmem, vmem],
            out_specs=[hbm] * 4,
            scratch_shapes=[pltpu.VMEM((nq + 2 * nk, D), F32), dma((STRIPS + 1, 3))],
            compiler_params=pltpu.CompilerParams(vmem_limit_bytes=16 * 1024 * 1024),
            name="widen",
        )(gw, din)
        return din, *grads

    return body


def solution(mesh):
    Z, X, Y, C = 8, 4, mesh.shape["dp"] // 2, 2
    finer = Mesh(mesh.devices.reshape(Z, X, Y, C), ("z", "x", "y", "c"))
    sp, dp = ("z", "x"), ("y", "c")
    return jax.shard_map(
        make_body(Z, X, Y, C),
        mesh=finer,
        in_specs=(P(sp, None), P(dp, None), P(dp, None), P(dp, None), P(), P(), P(sp, dp)),
        out_specs=(P(sp, dp), P(dp, None), P(dp, None), P(dp, None)),
        check_vma=False,
    )
```
